512 devices in a mesh: fs: 64 (over z, y), tp: 8 (over x, core).
Axes of the slice: x: 4, y: 8, z: 8, core: 2. Of those that a mesh axis runs over, the one named last changes fastest.
Arguments:
- late_input: bfloat16 [8192, 2048], P('fs', 'tp'), may hold values from -6 to 6
- up_weight: bfloat16 [2048, 4096], P('tp', 'fs'), may hold values from -0.125 to 0.125
- down_weight: bfloat16 [4096, 2048], P('fs', 'tp'), may hold values from -0.09375 to 0.09375
- early_input: bfloat16 [8192, 2048], P('fs', 'tp'), may hold values from -6 to 6
- early_pre: bfloat16 [8192, 4096], P('fs'), may hold values from -6 to 6
- cotangent: bfloat16 [8192, 2048], P('fs', 'tp'), may hold values from -16 to 16
- up_sum: float32 [2048, 4096], P('tp', 'fs'), may hold values from -24 to 24
- down_sum: float32 [4096, 2048], P('fs', 'tp'), may hold values from -24 to 24
Outputs:
- late_pre: bfloat16 [8192, 4096], P('fs')
- late_out: bfloat16 [8192, 2048], P('fs', 'tp')
- input_grad: bfloat16 [8192, 2048], P('fs', 'tp')
- up_total: float32 [2048, 4096], P('tp', 'fs')
- down_total: float32 [4096, 2048], P('fs', 'tp')
The draws below stay inside these ranges and needn't reach their ends.
All inputs are finite; a program needn't handle non-finite values.
Results may differ from the reference program's by a relative error of at most 0.025.
Values may be sent and summed in bfloat16 or wider, within the bound.
A program may use at most 128 MiB of HBM per device.

```python
import jax
import jax.numpy as jnp
from jax import lax

D = 2048
FF = 4096
TOKENS = 8192
DBLK = 256
N_TP = 8


def spiked(drawn, own_key, source, target, parts, factor):
    owner, partner = [(jnp.arange(drawn.shape[axis_at]) // (drawn.shape[axis_at] // parts)).reshape([-1 if axis == axis_at else 1 for axis in range(drawn.ndim)]) for axis_at in (source, target)]
    chosen = jax.random.permutation(own_key, parts)[partner]
    strong = (owner == chosen) | (owner == (partner + parts // 2) % parts)
    return jnp.where(strong, factor * drawn, drawn)


def steps_of(key, shape, split, smallest, largest):
    def one(position, shards_of):
        draws = jax.random.uniform(jax.random.fold_in(jax.random.fold_in(key, 6), position), (shards_of,), jnp.float32, smallest / len(split), largest / len(split))
        return jnp.repeat(jnp.exp(draws), shape[position] // shards_of).reshape((-1,) + (1,) * (len(shape) - position - 1))

    factor_of = one(*split[0])
    for cut in split[1:]:
        factor_of = factor_of * one(*cut)
    return factor_of


def centred(rng, shape, width, reach, split=(), held_as=jnp.bfloat16):
    loudness = steps_of(rng, shape, split, -0.22, 0.18) if split else 1.0
    values = jax.random.normal(rng, shape, jnp.float32) * width * loudness
    return jnp.minimum(jnp.maximum(values, -reach), reach).astype(held_as)


def bell_draw_with(key, shape, width, bound, pieces, heavy, held_as=jnp.bfloat16):
    values = width * jax.random.normal(key, shape, jnp.float32)
    if pieces:
        values = values * steps_of(key, shape, pieces, -0.22, 0.18)
    return jnp.clip(spiked(values, jax.random.fold_in(key, 3), *heavy), -bound, bound).astype(held_as)


def setup_inputs(seed: int = 0) -> dict:
    arg_keys = jax.random.split(jax.random.key(seed), 9)
    return {
        "late_input": centred(arg_keys[0], (TOKENS, D), 1.0, 6.0, ((0, 64), (1, 8))),
        "up_weight": centred(arg_keys[1], (D, FF), D ** -0.5, 0.125, ((0, 8), (1, 64))),
        "down_weight": centred(arg_keys[2], (FF, D), FF ** -0.5, 0.09375, ((0, 64), (1, 8))),
        "early_input": centred(arg_keys[3], (TOKENS, D), 1.0, 6.0, ((0, 64), (1, 8))),
        "early_pre": centred(arg_keys[4], (TOKENS, FF), 1.0, 6.0, ((0, 64),)),
        "cotangent": bell_draw_with(arg_keys[5], (TOKENS, D), 1.0, 16.0, ((0, 64), (1, 8)), (0, 1, 64, 4.0)),
        "up_sum": centred(arg_keys[6], (D, FF), 4.0, 24.0, ((0, 8), (1, 64)), jnp.float32),
        "down_sum": centred(arg_keys[7], (FF, D), 4.0, 24.0, ((0, 64), (1, 8)), jnp.float32),
    }


def block_sum(left, right):
    total = jnp.zeros((left.shape[0], right.shape[1]), jnp.float32)
    for block in range(N_TP):
        lower = block * DBLK
        partial_value = jnp.dot(left[:, lower:lower + DBLK], right[lower:lower + DBLK, :], preferred_element_type=jnp.float32)
        partial_value = lax.optimization_barrier(partial_value.astype(jnp.bfloat16))
        total = total + partial_value.astype(jnp.float32)
    return total


def reference(late_input, up_weight, down_weight, early_input, early_pre, cotangent, up_sum, down_sum):
    late_pre = block_sum(late_input, up_weight).astype(jnp.bfloat16)
    late_hidden = jnp.square(jax.nn.relu(late_pre.astype(jnp.float32))).astype(jnp.bfloat16)
    late_out = jnp.dot(late_hidden, down_weight, preferred_element_type=jnp.float32).astype(jnp.bfloat16)
    early_float = early_pre.astype(jnp.float32)
    early_hidden = jnp.square(jax.nn.relu(early_float)).astype(jnp.bfloat16)
    hidden_grad = block_sum(cotangent, down_weight.T)
    pre_grad = (hidden_grad * 2.0 * jax.nn.relu(early_float)).astype(jnp.bfloat16)
    input_grad = jnp.dot(pre_grad, up_weight.T, preferred_element_type=jnp.float32).astype(jnp.bfloat16)
    up_total = up_sum + jnp.dot(early_input.T, pre_grad, preferred_element_type=jnp.float32)
    down_total = down_sum + jnp.dot(early_hidden.T, cotangent, preferred_element_type=jnp.float32)
    return late_pre, late_out, input_grad, up_total, down_total
```

```python
import jax
import jax.numpy as jnp
from jax import lax
from jax.experimental import pallas as pl
from jax.experimental.pallas import tpu as pltpu
from jax.sharding import Mesh
from jax.sharding import PartitionSpec as P

FS = ("z", "y")
TP = ("x", "c")
MESH = pl.DeviceIdType.MESH
F32 = jnp.float32
BF16 = jnp.bfloat16
BLOCK_AXIS = ("z", "y")
SUB_AXIS = ("y", "z")


def nn(left, right):
    return lax.dot_general(left, right, (((1,), (0,)), ((), ())), preferred_element_type=F32)


def tn(left, right):
    return lax.dot_general(left, right, (((0,), (0,)), ((), ())), preferred_element_type=F32)


def square_relu(value):
    return jnp.square(jnp.maximum(value.astype(F32), 0.0)).astype(BF16)


def kernel(
    late_in, up_t, down, early_in, early_pre, cot, up_sum, down_sum,
    late_pre_o, late_out_o, input_grad_o, up_total_o, down_total_o,
    weights, grads, ring_in, last_in, early_t, cot_t, late_t, part, pair_in, pair_sum, x_in, full, acc,
    own_sem, ag1_s, ag1_r, ag2_s, ag2_r, rs1_s, rs1_r, rs2_s, rs2_r,
    pair_s, pair_r, xr_s, xr_r, xg_s, xg_r, cg_s, cg_r, fw_s, fw_r,
):
    iz, iy, ix, ic = (lax.axis_index(name) for name in ("z", "y", "x", "c"))
    place = (iz, iy)
    sub_place = (iy, iz)
    shards = (down, up_t)
    sent = []

    def up_by(value, step, size=8):
        return lax.rem(value + (step % size), size)

    def remote(src, dst, send_sem, recv_sem, axis, index):
        return pltpu.make_async_remote_copy(
            src_ref=src, dst_ref=dst, send_sem=send_sem, recv_sem=recv_sem,
            device_id={axis: index}, device_id_type=MESH,
        )

    def send(*args):
        copy = remote(*args)
        copy.start()
        sent.append(copy)

    barrier = pltpu.get_barrier_semaphore()
    for axis, me, size in (("y", iy, 8), ("z", iz, 8), ("x", ix, 4), ("c", ic, 2)):
        for step in range(1, size):
            pl.semaphore_signal(
                barrier, inc=1, device_id={axis: up_by(me, step, size)}, device_id_type=MESH
            )
    pl.semaphore_wait(barrier, 18)

    own = []

    def ag1_send(w):
        for h in range(2):
            rows = shards[w].at[pl.ds(32 * h, 32), :]
            target = weights.at[w, h, place[h], sub_place[h]]
            copy = pltpu.make_async_copy(rows, target, own_sem.at[w, h])
            copy.start()
            own.append(copy)
            for step in (4, 3, 5, 2, 6, 1, 7):
                send(
                    rows, target, ag1_s.at[w, h, step - 1], ag1_r.at[w, h, step - 1],
                    SUB_AXIS[h], up_by(sub_place[h], step),
                )

    def ag1_wait(w):
        for h in range(2):
            own[2 * w + h].wait()
            for step in range(1, 8):
                target = weights.at[w, h, place[h], up_by(sub_place[h], -step)]
                remote(
                    target, target, ag1_s.at[w, h, step - 1], ag1_r.at[w, h, step - 1],
                    SUB_AXIS[h], up_by(sub_place[h], -step),
                ).wait_recv()

    def ag2_piece(w, h, way, step, part_at, arriving):
        sign = 1 - 2 * way
        away = -sign * (step if arriving else step - 1)
        ref = weights.at[w, h, up_by(place[h], away), pl.ds(4 * part_at, 4)]
        at = (w, h, way, step - 1, part_at)
        return ref, ref, ag2_s.at[at], ag2_r.at[at], BLOCK_AXIS[h], up_by(place[h], sign)

    def ag2_has(step, way, part_at):
        return step < 4 or part_at == way

    def ag2_start(w):
        for part_at in range(2):
            for h in range(2):
                for way in range(2):
                    send(*ag2_piece(w, h, way, 1, part_at, False))

    def ag2_step(w, step):
        for part_at in range(2):
            for h in range(2):
                for way in range(2):
                    if ag2_has(step, way, part_at):
                        remote(*ag2_piece(w, h, way, step, part_at, True)).wait_recv()
                        if step < 4 and ag2_has(step + 1, way, part_at):
                            send(*ag2_piece(w, h, way, step + 1, part_at, False))

    def rs_send(w, h, way, step, part_at):
        sign = 1 - 2 * way
        at = (w, h, way, step - 1, part_at)
        send(
            grads.at[w, h, up_by(place[h], sign * (5 - step)), pl.ds(4 * part_at, 4)],
            ring_in.at[w, h, way, step - 1, pl.ds(4 * part_at, 4)],
            rs1_s.at[at], rs1_r.at[at], BLOCK_AXIS[h], up_by(place[h], sign),
        )

    def rs_wait(w, h, way, step, part_at):
        sign = 1 - 2 * way
        at = (w, h, way, step - 1, part_at)
        ref = ring_in.at[w, h, way, step - 1, pl.ds(4 * part_at, 4)]
        remote(ref, ref, rs1_s.at[at], rs1_r.at[at], BLOCK_AXIS[h], up_by(place[h], sign)).wait_recv()
        return ref

    def rs_start(w):
        for h in range(2):
            for way in range(2):
                rs_send(w, h, way, 1, way)
        for h in range(2):
            for way in range(2):
                rs_send(w, h, way, 2, 1 - way)

    def rs_step(w, step):
        for part_at in range(2):
            for h in range(2):
                for way in range(2):
                    if step == 1 and part_at != way:
                        continue
                    arrived = rs_wait(w, h, way, step, part_at)
                    block = up_by(place[h], (1 - 2 * way) * (4 - step))
                    mine = grads.at[w, h, block, pl.ds(4 * part_at, 4)]
                    mine[...] = (mine[...].astype(F32) + arrived[...].astype(F32)).astype(BF16)
                    rs_send(w, h, way, step + 1, part_at)

    def rs_last(w):
        for part_at in range(2):
            for h in range(2):
                mine = grads.at[w, h, place[h], pl.ds(4 * part_at, 4)]
                total = mine[...].astype(F32)
                for way in range(2):
                    total = total + rs_wait(w, h, way, 4, part_at)[...].astype(F32)
                mine[...] = total.astype(BF16)
        for h in range(2):
            for step in (4, 3, 5, 2, 6, 1, 7):
                send(
                    grads.at[w, h, place[h], up_by(sub_place[h], step)], last_in.at[w, h, step - 1],
                    rs2_s.at[w, h, step - 1], rs2_r.at[w, h, step - 1],
                    SUB_AXIS[h], up_by(sub_place[h], step),
                )

    def rs_out(w):
        base, out = ((down_sum, down_total_o), (up_sum, up_total_o))[w]
        for h in range(2):
            total = grads[w, h, place[h], sub_place[h]].astype(F32)
            for step in range(1, 8):
                ref = last_in.at[w, h, step - 1]
                remote(
                    ref, ref, rs2_s.at[w, h, step - 1], rs2_r.at[w, h, step - 1],
                    SUB_AXIS[h], up_by(sub_place[h], step),
                ).wait_recv()
                total = total + ref[...].astype(F32)
            rows = pl.ds(32 * h, 32)
            out[rows, :] = base[rows, :] + total

    def block_of(h, side, j):
        return lax.rem(iz * (1 - h) + iy * h + side * (2 * j + 1) - j + 8, 8)

    def product(a, j, sides):
        w, right = ((0, cot_t), (1, late_t))[a]

        def one(h, _):
            for side in sides:
                rows = weights[w, h, block_of(h, side, j)].reshape(256, 256)
                part[a, j, pl.ds(pl.multiple_of(h * 512 + side * 256, 256), 256), :] = nn(
                    rows, right[...]
                ).astype(BF16)
            return 0

        lax.fori_loop(0, 2, one, 0)

    other = up_by(ic, 1, 2)
    my_half = pl.multiple_of(ic * 512, 512)
    other_half = pl.multiple_of(other * 512, 512)

    def s1(a, j):
        send(
            part.at[a, j, pl.ds(other_half, 512), :], pair_in.at[a, j],
            pair_s.at[a, j], pair_r.at[a, j], "c", other,
        )

    def s2(a, j):
        ref = pair_in.at[a, j]
        remote(ref, ref, pair_s.at[a, j], pair_r.at[a, j], "c", other).wait_recv()
        pair_sum[a, j] = (
            part[a, j, pl.ds(my_half, 512), :].astype(F32) + pair_in[a, j].astype(F32)
        ).astype(BF16)
        for step in (2, 1, 3):
            target = up_by(ix, step, 4)
            rows = pl.ds(pl.multiple_of(target * 128, 128), 128)
            at = (a, j, step - 1)
            send(pair_sum.at[a, j, rows, :], x_in.at[at], xr_s.at[at], xr_r.at[at], "x", target)

    def rows_of(core, x):
        return pl.ds(pl.multiple_of(core * 512 + x * 128, 128), 128)

    def s3(a, j):
        total = pair_sum[a, j, pl.ds(pl.multiple_of(ix * 128, 128), 128), :].astype(F32)
        for step in (1, 3, 2):
            at = (a, j, step - 1)
            ref = x_in.at[at]
            remote(ref, ref, xr_s.at[at], xr_r.at[at], "x", up_by(ix, step, 4)).wait_recv()
            total = total + ref[...].astype(F32)
        mine = rows_of(ic, ix)
        if a == 0:
            block = block_of(ic, ix // 2, j)
            saved = early_t[ic, block, pl.ds(4 * lax.rem(ix, 2), 4)].reshape(128, 128)
            total = total * 2.0 * jnp.maximum(saved.astype(F32), 0.0)
        full[a, j, mine, :] = total.astype(BF16)
        ref = full.at[a, j, mine, :]
        for step in (2, 1, 3):
            at = (a, j, step - 1)
            send(ref, ref, xg_s.at[at], xg_r.at[at], "x", up_by(ix, step, 4))
        send(ref, ref, cg_s.at[a, j], cg_r.at[a, j], "c", other)

    def s4(a, j):
        for step in (1, 3, 2):
            at = (a, j, step - 1)
            source = up_by(ix, -step, 4)
            ref = full.at[a, j, rows_of(ic, source), :]
            remote(ref, ref, xg_s.at[at], xg_r.at[at], "x", source).wait_recv()
            send(ref, ref, fw_s.at[at], fw_r.at[at], "c", other)

    def s5(a, j):
        ref = full.at[a, j, rows_of(other, ix), :]
        remote(ref, ref, cg_s.at[a, j], cg_r.at[a, j], "c", other).wait_recv()
        for step in (1, 3, 2):
            at = (a, j, step - 1)
            ref = full.at[a, j, rows_of(other, up_by(ix, -step, 4)), :]
            remote(ref, ref, fw_s.at[at], fw_r.at[at], "c", other).wait_recv()

    def pieces(j, fn):
        def one(at, _):
            h, side = at // 2, lax.rem(at, 2)
            fn(h, block_of(h, side, j), pl.ds(pl.multiple_of(at * 256, 256), 256))
            return 0

        lax.fori_loop(0, 4, one, 0)

    def up_grads(j):
        def fn(h, block, rows):
            grads[1, h, block] = nn(full[0, j, rows, :], early_in[...]).astype(BF16).reshape(8, 32, 256)

        pieces(j, fn)

    def input_grads(j):
        def fn(h, block, rows):
            acc[0] += tn(full[0, j, rows, :], weights[1, h, block].reshape(256, 256))

        pieces(j, fn)

    def late_outs(j):
        def fn(h, block, rows):
            acc[1] += tn(square_relu(full[1, j, rows, :]), weights[0, h, block].reshape(256, 256))
            for sub in range(8):
                early_t[h, block, sub] = full[1, j, pl.ds(rows.start + 32 * sub, 32), :]

        pieces(j, fn)

    def turn_early(at, _):
        z, y = at // 4, 2 * lax.rem(at, 4)
        turned = early_pre[:, pl.ds(pl.multiple_of(at * 128, 128), 128)].T
        early_t[0, z, y] = turned[0:32]
        early_t[1, y, z] = turned[32:64]
        early_t[0, z, y + 1] = turned[64:96]
        early_t[1, y + 1, z] = turned[96:128]
        return 0

    def turn_late(at, _):
        z, y = at // 4, 2 * lax.rem(at, 4)
        rows = jnp.concatenate(
            [early_t[0, z, y], early_t[1, y, z], early_t[0, z, y + 1], early_t[1, y + 1, z]], axis=0
        )
        late_pre_o[:, pl.ds(pl.multiple_of(at * 128, 128), 128)] = rows.T
        return 0

    def down_grads(at, _):
        h, block = at // 8, lax.rem(at, 8)
        hidden = square_relu(early_t[h, block].reshape(256, 128))
        grads[0, h, block] = nn(hidden, cot[...]).astype(BF16).reshape(8, 32, 256)
        return 0

    ag1_send(0)
    ag1_send(1)
    cot_t[...] = cot[...].T
    late_t[...] = late_in[...].T
    acc[...] = jnp.zeros_like(acc)
    lax.fori_loop(0, 32, turn_early, 0)
    ag1_wait(0)
    ag2_start(0)
    product(0, 0, (0,))
    lax.fori_loop(0, 16, down_grads, 0)
    ag2_step(0, 1)
    product(0, 0, (1,))
    s1(0, 0)
    product(0, 1, (0,))
    s2(0, 0)
    ag2_step(0, 2)
    product(0, 1, (1,))
    s1(0, 1)
    product(0, 2, (0,))
    s2(0, 1)
    ag2_step(0, 3)
    ag1_wait(1)
    ag2_start(1)
    product(0, 2, (1,))
    s1(0, 2)
    product(0, 3, (0,))
    s3(0, 0)
    s2(0, 2)
    ag2_step(0, 4)
    product(0, 3, (1,))
    s1(0, 3)
    s3(0, 1)
    s4(0, 0)
    s2(0, 3)
    s3(0, 2)
    ag2_step(1, 1)
    s5(0, 0)
    s4(0, 1)
    up_grads(0)
    s3(0, 3)
    ag2_step(1, 2)
    s5(0, 1)
    s4(0, 2)
    up_grads(1)
    ag2_step(1, 3)
    rs_start(0)
    s5(0, 2)
    s4(0, 3)
    up_grads(2)
    s5(0, 3)
    up_grads(3)
    rs_start(1)
    ag2_step(1, 4)
    for j in range(4):
        product(1, j, (0, 1))
        s1(1, j)
    rs_step(0, 1)
    for j in range(4):
        s2(1, j)
    rs_step(1, 1)
    rs_step(0, 2)
    s3(1, 0)
    s3(1, 1)
    rs_step(1, 2)
    s3(1, 2)
    s3(1, 3)
    rs_step(0, 3)
    s4(1, 0)
    s4(1, 1)
    rs_step(1, 3)
    s4(1, 2)
    s4(1, 3)
    rs_last(0)
    for j in range(4):
        s5(1, j)
        late_outs(j)
    rs_last(1)
    for j in range(4):
        input_grads(j)
    late_out_o[...] = acc[1].astype(BF16)
    input_grad_o[...] = acc[0].astype(BF16)
    lax.fori_loop(0, 32, turn_late, 0)
    rs_out(0)
    rs_out(1)
    for copy in sent:
        copy.wait_send()


def body(late_input, up_weight, down_weight, early_input, early_pre, cotangent, up_sum, down_sum):
    vmem = pl.BlockSpec(memory_space=pltpu.VMEM)
    dma = pltpu.SemaphoreType.DMA
    outs = pl.pallas_call(
        kernel,
        out_shape=(
            jax.ShapeDtypeStruct((128, 4096), BF16),
            jax.ShapeDtypeStruct((128, 256), BF16),
            jax.ShapeDtypeStruct((128, 256), BF16),
            jax.ShapeDtypeStruct((64, 256), F32),
            jax.ShapeDtypeStruct((64, 256), F32),
        ),
        in_specs=[vmem] * 8,
        out_specs=(vmem,) * 5,
        scratch_shapes=[
            pltpu.VMEM((2, 2, 8, 8, 32, 256), BF16),
            pltpu.VMEM((2, 2, 8, 8, 32, 256), BF16),
            pltpu.VMEM((2, 2, 2, 4, 8, 32, 256), BF16),
            pltpu.VMEM((2, 2, 7, 32, 256), BF16),
            pltpu.VMEM((2, 8, 8, 32, 128), BF16),
            pltpu.VMEM((256, 128), BF16),
            pltpu.VMEM((256, 128), BF16),
            pltpu.VMEM((2, 4, 1024, 128), BF16),
            pltpu.VMEM((2, 4, 512, 128), BF16),
            pltpu.VMEM((2, 4, 512, 128), BF16),
            pltpu.VMEM((2, 4, 3, 128, 128), BF16),
            pltpu.VMEM((2, 4, 1024, 128), BF16),
            pltpu.VMEM((2, 128, 256), F32),
            dma((2, 2)),
            dma((2, 2, 7)), dma((2, 2, 7)),
            dma((2, 2, 2, 4, 2)), dma((2, 2, 2, 4, 2)),
            dma((2, 2, 2, 4, 2)), dma((2, 2, 2, 4, 2)),
            dma((2, 2, 7)), dma((2, 2, 7)),
            dma((2, 4)), dma((2, 4)),
            dma((2, 4, 3)), dma((2, 4, 3)),
            dma((2, 4, 3)), dma((2, 4, 3)),
            dma((2, 4)), dma((2, 4)),
            dma((2, 4, 3)), dma((2, 4, 3)),
        ],
        compiler_params=pltpu.CompilerParams(
            collective_id=0, has_side_effects=True, vmem_limit_bytes=60 * 1024 * 1024
        ),
        cost_estimate=pl.CostEstimate(flops=1_700_000_000, bytes_accessed=8_000_000, transcendentals=0),
    )(late_input, up_weight.T, down_weight, early_input, early_pre, cotangent, up_sum.T, down_sum)
    late_pre, late_out, input_grad, up_total, down_total = outs
    return late_pre, late_out, input_grad, up_total.T, down_total


def solution(mesh):
    split = Mesh(mesh.devices.reshape(8, 8, 4, 2), FS + TP)
    placed = (
        P(FS, TP), P(TP, FS), P(FS, TP), P(FS, TP), P(FS, None), P(FS, TP), P(TP, FS), P(FS, TP),
    )
    return jax.shard_map(
        body,
        mesh=split,
        in_specs=placed,
        out_specs=(P(FS, None), P(FS, TP), P(FS, TP), P(TP, FS), P(FS, TP)),
        check_vma=False,
    )
```

```python
import jax
import jax.numpy as jnp
from jax import lax
from jax.experimental import pallas as pl
from jax.experimental.pallas import tpu as pltpu
from jax.sharding import Mesh
from jax.sharding import PartitionSpec as P

FS = ("z", "y")
TP = ("x", "c")
MESH = pl.DeviceIdType.MESH
F32 = jnp.float32
BF16 = jnp.bfloat16
BLOCK_AXIS = ("z", "y")
SUB_AXIS = ("y", "z")


def nn(left, right):
    return lax.dot_general(left, right, (((1,), (0,)), ((), ())), preferred_element_type=F32)


def tn(left, right):
    return lax.dot_general(left, right, (((0,), (0,)), ((), ())), preferred_element_type=F32)


def square_relu(value):
    return jnp.square(jnp.maximum(value.astype(F32), 0.0)).astype(BF16)


def kernel(
    late_in_h, up_t_h, down_h, early_in_h, early_pre_h, cot_h, up_sum_h, down_sum_h,
    late_pre_o, late_out_o, input_grad_o, up_total_o, down_total_o,
    late_in, up_t, down, early_in, early_pre, cot, up_sum, down_sum, weights, grads, ring_in, last_in, early_t, cot_t, late_t, part, pair_in, pair_sum, x_in, full, acc,
    in_sem, own_sem, ag1_s, ag1_r, ag2_s, ag2_r, rs1_s, rs1_r, rs2_s, rs2_r,
    tp_s, pair_r, xr_r, xg_r, fw_r,
):
    iz, iy, ix, ic = (lax.axis_index(name) for name in ("z", "y", "x", "c"))
    place = (iz, iy)
    sub_place = (iy, iz)
    shards = (down, up_t)

    def up_by(value, step, size=8):
        return lax.rem(value + (step % size), size)

    def send(src, dst, send_sem, recv_sem, axis, index):
        pltpu.make_async_remote_copy(
            src_ref=src, dst_ref=dst, send_sem=send_sem, recv_sem=recv_sem,
            device_id={axis: index}, device_id_type=MESH,
        ).start()

    def arrive(ref, recv_sem):
        pltpu.make_async_remote_copy(
            src_ref=ref, dst_ref=ref, send_sem=recv_sem, recv_sem=recv_sem,
            device_id={"c": up_by(ic, 1, 2)}, device_id_type=MESH,
        ).wait_recv()

    def gone(ref, send_sem):
        pltpu.make_async_remote_copy(
            src_ref=ref, dst_ref=ref, send_sem=send_sem, recv_sem=send_sem,
            device_id={"c": up_by(ic, 1, 2)}, device_id_type=MESH,
        ).wait_send()

    barrier = pltpu.get_barrier_semaphore()
    for axis, me, size in (("y", iy, 8), ("z", iz, 8), ("x", ix, 4), ("c", ic, 2)):
        for step in range(1, size):
            pl.semaphore_signal(
                barrier, inc=1, device_id={axis: up_by(me, step, size)}, device_id_type=MESH
            )
    loads = []
    for at, (source, target) in enumerate((
        (down_h, down), (up_t_h, up_t), (cot_h, cot), (late_in_h, late_in), (early_pre_h, early_pre),
        (early_in_h, early_in), (down_sum_h, down_sum), (up_sum_h, up_sum),
    )):
        copy = pltpu.make_async_copy(source, target, in_sem.at[at])
        copy.start()
        loads.append(copy)
    loads[0].wait()
    pl.semaphore_wait(barrier, 18)

    own = []

    def own_copy(w):
        if w == 1:
            loads[1].wait()
        for h in range(2):
            rows = shards[w].at[pl.ds(32 * h, 32), :]
            copy = pltpu.make_async_copy(rows, weights.at[w, h, place[h], sub_place[h]], own_sem.at[w, h])
            copy.start()
            own.append(copy)

    def ag1_send(w):
        for step in (4, 3, 5, 2, 6, 1, 7):
            for h in range(2):
                rows = shards[w].at[pl.ds(32 * h, 32), :]
                target = weights.at[w, h, place[h], sub_place[h]]
                send(rows, target, ag1_s.at[w], ag1_r.at[0], SUB_AXIS[h], up_by(sub_place[h], step))

    def ag1_wait(w):
        for h in range(2):
            own[2 * w + h].wait()
        arrive(weights.at[w, 0, pl.ds(0, 7), pl.ds(0, 2)], ag1_r.at[0])

    def ring_send(w, h, way, step):
        sign = (1 - 2 * way) * (1 - 2 * h)
        ref = weights.at[w, h, place[h], up_by(sub_place[h], -sign * (step - 1))]
        send(ref, ref, ag1_s.at[w], ag1_r.at[step], SUB_AXIS[h], up_by(sub_place[h], sign))

    def ag1_ring_start(w):
        for h in range(2):
            own[2 * w + h].wait()
            for way in range(2):
                ring_send(w, h, way, 1)

    def ag1_ring_step(w, step):
        arrive(weights.at[w, 0, 0, pl.ds(0, 4 if step < 4 else 2)], ag1_r.at[step])
        for h in range(2):
            for way in range(2):
                if step + way < 4:
                    ring_send(w, h, way, step + 1)

    def ag2_send(w, h, way, step, part_at):
        sign = 1 - 2 * way
        ref = weights.at[w, h, up_by(place[h], -sign * (step - 1)), pl.ds(4 * part_at, 4)]
        send(ref, ref, ag2_s.at[w, h], ag2_r.at[w, h, step - 1, part_at], BLOCK_AXIS[h], up_by(place[h], sign))

    def ag2_start(w):
        for part_at in range(2):
            for h in range(2):
                for way in range(2):
                    ag2_send(w, h, way, 1, part_at)

    def ag2_part(w, step, part_at):
        for h in range(2):
            size = 8 if step < 4 else 4
            arrive(weights.at[w, h, 0, pl.ds(0, size)], ag2_r.at[w, h, step - 1, part_at])
            for way in range(2):
                if step < 3 or (step == 3 and part_at == way):
                    ag2_send(w, h, way, step + 1, part_at)

    def rs_send(w, h, way, step, part_at):
        sign = 1 - 2 * way
        send(
            grads.at[w, h, up_by(place[h], sign * (5 - step)), pl.ds(4 * part_at, 4)],
            ring_in.at[w, h, way, step - 1, pl.ds(4 * part_at, 4)],
            rs1_s.at[w, h], rs1_r.at[w, h, step - 1, part_at], BLOCK_AXIS[h], up_by(place[h], sign),
        )

    def rs_start(w):
        for h in range(2):
            for way in range(2):
                rs_send(w, h, way, 1, way)
        for h in range(2):
            for way in range(2):
                rs_send(w, h, way, 2, 1 - way)

    def rs_part(w, step, part_at):
        for h in range(2):
            size = 8 if step > 1 else 4
            arrive(weights.at[w, h, 0, pl.ds(0, size)], rs1_r.at[w, h, step - 1, part_at])
            for way in range(2):
                if step == 1 and part_at != way:
                    continue
                arrived = ring_in.at[w, h, way, step - 1, pl.ds(4 * part_at, 4)]
                block = up_by(place[h], (1 - 2 * way) * (4 - step))
                mine = grads.at[w, h, block, pl.ds(4 * part_at, 4)]
                mine[...] = (mine[...].astype(F32) + arrived[...].astype(F32)).astype(BF16)
                rs_send(w, h, way, step + 1, part_at)

    def rs_last(w, part_at):
        for h in range(2):
            arrive(weights.at[w, h, 0], rs1_r.at[w, h, 3, part_at])
            mine = grads.at[w, h, place[h], pl.ds(4 * part_at, 4)]
            total = mine[...].astype(F32)
            for way in range(2):
                total = total + ring_in[w, h, way, 3, pl.ds(4 * part_at, 4)].astype(F32)
            mine[...] = total.astype(BF16)

    def rs2_send(w):
        for step in (4, 3, 5, 2, 6, 1, 7):
            for h in range(2):
                send(
                    grads.at[w, h, place[h], up_by(sub_place[h], step)], last_in.at[w, h, step - 1],
                    rs2_s.at[w], rs2_r.at[0], SUB_AXIS[h], up_by(sub_place[h], step),
                )

    def rs2_ring_send(w, h, way, step):
        sign = (1 - 2 * way) * (1 - 2 * h)
        send(
            grads.at[w, h, place[h], up_by(sub_place[h], sign * (5 - way - step))],
            last_in.at[w, h, 4 * way + step - 1],
            rs2_s.at[w], rs2_r.at[step], SUB_AXIS[h], up_by(sub_place[h], sign),
        )

    def rs2_ring_start(w):
        for h in range(2):
            for way in range(2):
                rs2_ring_send(w, h, way, 1)

    def rs2_ring_step(w, step):
        arrive(weights.at[w, 0, 0, pl.ds(0, 4)], rs2_r.at[step])
        for h in range(2):
            for way in range(2):
                if step + way < 4:
                    sign = (1 - 2 * way) * (1 - 2 * h)
                    mine = grads.at[w, h, place[h], up_by(sub_place[h], sign * (4 - way - step))]
                    arrived = last_in[w, h, 4 * way + step - 1]
                    mine[...] = (mine[...].astype(F32) + arrived.astype(F32)).astype(BF16)
                    rs2_ring_send(w, h, way, step + 1)

    def rs_out(w, ring):
        base, out = ((down_sum, down_total_o), (up_sum, up_total_o))[w]
        if ring:
            arrive(weights.at[w, 0, 0, pl.ds(0, 2)], rs2_r.at[4])
        else:
            arrive(weights.at[w, 0, pl.ds(0, 7), pl.ds(0, 2)], rs2_r.at[0])
        for h in range(2):
            total = grads[w, h, place[h], sub_place[h]].astype(F32)
            for at in (3, 6) if ring else range(7):
                total = total + last_in[w, h, at].astype(F32)
            rows = pl.ds(32 * h, 32)
            out[rows, :] = base[rows, :] + total

    def block_of(h, side, j):
        return lax.rem(iz * (1 - h) + iy * h + side * (2 * j + 1) - j + 8, 8)

    def product(a, j, sides):
        w, right = ((0, cot_t), (1, late_t))[a]

        def one(h, _):
            for side in sides:
                rows = weights[w, h, block_of(h, side, j)].reshape(256, 256)
                part[a, j, pl.ds(pl.multiple_of(h * 512 + side * 256, 256), 256), :] = nn(
                    rows, right[...]
                ).astype(BF16)
            return 0

        lax.fori_loop(0, 2, one, 0)

    other = up_by(ic, 1, 2)
    my_half = pl.multiple_of(ic * 512, 512)
    other_half = pl.multiple_of(other * 512, 512)

    def s1(a, j):
        send(
            part.at[a, j, pl.ds(other_half, 512), :], pair_in.at[a, j],
            tp_s.at[a, 0], pair_r.at[a, j], "c", other,
        )

    def s2(a, j):
        arrive(pair_in.at[a, j], pair_r.at[a, j])
        pair_sum[a, j] = (
            part[a, j, pl.ds(my_half, 512), :].astype(F32) + pair_in[a, j].astype(F32)
        ).astype(BF16)
        for step in (2, 1, 3):
            target = up_by(ix, step, 4)
            rows = pl.ds(pl.multiple_of(target * 128, 128), 128)
            send(pair_sum.at[a, j, rows, :], x_in.at[a, j, step - 1], tp_s.at[a, 1], xr_r.at[a, j], "x", target)

    def share(a, core, x, j):
        return full.at[a, core, block_of(core, x // 2, j), pl.ds(4 * lax.rem(x, 2), 4)]

    def s3(a, j):
        total = pair_sum[a, j, pl.ds(pl.multiple_of(ix * 128, 128), 128), :].astype(F32)
        arrive(x_in.at[a, j], xr_r.at[a, j])
        for at in range(3):
            total = total + x_in[a, j, at].astype(F32)
        if a == 0:
            block = block_of(ic, ix // 2, j)
            saved = early_t[ic, block, pl.ds(4 * lax.rem(ix, 2), 4)].reshape(128, 128)
            total = total * 2.0 * jnp.maximum(saved.astype(F32), 0.0)
        ref = share(a, ic, ix, j)
        ref[...] = total.astype(BF16).reshape(4, 32, 128)
        for step in (2, 1, 3):
            send(ref, ref, tp_s.at[a, 2], xg_r.at[a, j], "x", up_by(ix, step, 4))
        send(ref, ref, tp_s.at[a, 3], fw_r.at[a, j], "c", other)

    def s4(a, j):
        arrive(x_in.at[a, j], xg_r.at[a, j])
        for step in (1, 2, 3):
            ref = share(a, ic, up_by(ix, step, 4), j)
            send(ref, ref, tp_s.at[a, 3], fw_r.at[a, j], "c", other)

    def s5(a, j):
        arrive(pair_in.at[a, j], fw_r.at[a, j])

    def all_gone():
        small = weights.at[0, 0, pl.ds(0, 7), pl.ds(0, 2)]
        for w in range(2):
            gone(small, ag1_s.at[w])
            gone(small, rs2_s.at[w])
            for h in range(2):
                gone(weights.at[w, h, pl.ds(0, 7)], ag2_s.at[w, h])
                gone(weights.at[w, h, pl.ds(0, 7)], rs1_s.at[w, h])
            gone(pair_in.at[w], tp_s.at[w, 0])
            gone(x_in.at[w], tp_s.at[w, 1])
            gone(x_in.at[w], tp_s.at[w, 2])
            gone(pair_in.at[w], tp_s.at[w, 3])

    def pieces(j, fn):
        def one(at, _):
            h, side = at // 2, lax.rem(at, 2)
            fn(h, block_of(h, side, j))
            return 0

        lax.fori_loop(0, 4, one, 0)

    def up_grads(j):
        def fn(h, block):
            rows = full[0, h, block].reshape(256, 128)
            grads[1, h, block] = nn(rows, early_in[...]).astype(BF16).reshape(8, 32, 256)

        pieces(j, fn)

    def input_grads(j):
        def fn(h, block):
            acc[0] += tn(full[0, h, block].reshape(256, 128), weights[1, h, block].reshape(256, 256))

        pieces(j, fn)

    def late_outs(j):
        def fn(h, block):
            hidden = square_relu(full[1, h, block].reshape(256, 128))
            acc[1] += tn(hidden, weights[0, h, block].reshape(256, 256))

        pieces(j, fn)

    def early(quarter):
        def one(at, _):
            z, y = at // 4, 2 * lax.rem(at, 4)
            turned = early_pre[:, pl.ds(pl.multiple_of(at * 128, 128), 128)].T
            early_t[0, z, y] = turned[0:32]
            early_t[1, y, z] = turned[32:64]
            early_t[0, z, y + 1] = turned[64:96]
            early_t[1, y + 1, z] = turned[96:128]
            return 0

        if quarter == 0:
            loads[4].wait()
        lax.fori_loop(8 * quarter, 8 * quarter + 8, one, 0)

    def turn_late(quarter):
        def one(at, _):
            z, y = at // 4, 2 * lax.rem(at, 4)
            rows = jnp.concatenate(
                [full[1, 0, z, y], full[1, 1, y, z], full[1, 0, z, y + 1], full[1, 1, y + 1, z]], axis=0
            )
            late_pre_o[:, pl.ds(pl.multiple_of(at * 128, 128), 128)] = rows.T
            return 0

        lax.fori_loop(8 * quarter, 8 * quarter + 8, one, 0)

    def down_grads(j):
        def fn(h, block):
            hidden = square_relu(early_t[h, block].reshape(256, 128))
            grads[0, h, block] = nn(hidden, cot[...]).astype(BF16).reshape(8, 32, 256)

        pieces(j, fn)

    def prep_cot():
        loads[2].wait()
        cot_t[...] = cot[...].T

    def prep_late():
        loads[3].wait()
        late_t[...] = late_in[...].T
        acc[...] = jnp.zeros_like(acc)
        loads[5].wait()
        loads[6].wait()
        loads[7].wait()

    def fin_late():
        late_out_o[...] = acc[1].astype(BF16)

    def fin_input():
        input_grad_o[...] = acc[0].astype(BF16)

    own_copy(0)
    ag1_send(0)
    own_copy(1)
    early(0)
    early(1)
    early(2)
    early(3)
    prep_cot()
    down_grads(1)
    down_grads(3)
    down_grads(0)
    ag1_wait(0)
    ag2_start(0)
    product(0, 0, (0,))
    ag1_ring_start(1)
    prep_late()
    down_grads(2)
    rs_start(0)
    ag2_part(0, 1, 0)
    ag2_part(0, 1, 1)
    product(0, 0, (1,))
    s1(0, 0)
    ag1_ring_step(1, 1)
    product(0, 1, (0,))
    rs_part(0, 1, 1)
    rs_part(0, 1, 0)
    s2(0, 0)
    ag2_part(0, 2, 0)
    ag2_part(0, 2, 1)
    product(0, 1, (1,))
    ag1_ring_step(1, 2)
    s1(0, 1)
    product(0, 2, (0,))
    s3(0, 0)
    s2(0, 1)
    rs_part(0, 2, 0)
    rs_part(0, 2, 1)
    ag2_part(0, 3, 0)
    ag2_part(0, 3, 1)
    product(0, 3, (0,))
    ag1_ring_step(1, 3)
    product(0, 2, (1,))
    s1(0, 2)
    s4(0, 0)
    rs_part(0, 3, 0)
    s2(0, 2)
    s5(0, 0)
    up_grads(0)
    s3(0, 1)
    rs_part(0, 3, 1)
    ag2_part(0, 4, 0)
    ag2_part(0, 4, 1)
    product(0, 3, (1,))
    s1(0, 3)
    ag1_ring_step(1, 4)
    ag2_start(1)
    product(1, 0, (0,))
    s2(0, 3)
    rs_last(0, 0)
    s3(0, 2)
    rs_last(0, 1)
    rs2_ring_start(0)
    s4(0, 1)
    ag2_part(1, 1, 0)
    s5(0, 1)
    up_grads(1)
    ag2_part(1, 1, 1)
    product(1, 1, (0,))
    s3(0, 3)
    rs2_ring_step(0, 1)
    product(1, 0, (1,))
    s1(1, 0)
    s4(0, 2)
    ag2_part(1, 2, 0)
    s2(1, 0)
    s5(0, 2)
    up_grads(2)
    rs2_ring_step(0, 2)
    ag2_part(1, 2, 1)
    product(1, 2, (0,))
    product(1, 1, (1,))
    s4(0, 3)
    s1(1, 1)
    ag2_part(1, 3, 0)
    s5(0, 3)
    up_grads(3)
    rs_start(1)
    rs2_ring_step(0, 3)
    s2(1, 1)
    s3(1, 0)
    ag2_part(1, 3, 1)
    product(1, 2, (1,))
    s1(1, 2)
    product(1, 3, (0,))
    ag2_part(1, 4, 0)
    s2(1, 2)
    rs_part(1, 1, 1)
    rs_part(1, 1, 0)
    s3(1, 1)
    rs_out(0, True)
    ag2_part(1, 4, 1)
    product(1, 3, (1,))
    s1(1, 3)
    input_grads(2)
    input_grads(3)
    rs_part(1, 2, 0)
    s2(1, 3)
    rs_part(1, 2, 1)
    s4(1, 0)
    input_grads(0)
    s3(1, 2)
    input_grads(1)
    s5(1, 0)
    late_outs(0)
    s4(1, 1)
    fin_input()
    rs_part(1, 3, 0)
    s5(1, 1)
    late_outs(1)
    s3(1, 3)
    rs_part(1, 3, 1)
    s4(1, 2)
    rs_last(1, 0)
    s5(1, 2)
    late_outs(2)
    rs_last(1, 1)
    rs2_send(1)
    s4(1, 3)
    s5(1, 3)
    turn_late(2)
    late_outs(3)
    turn_late(1)
    fin_late()
    turn_late(3)
    turn_late(0)
    rs_out(1, False)
    all_gone()


def deliver(*refs):
    sources, targets, sems = refs[:5], refs[5:10], refs[10]
    copies = [pltpu.make_async_copy(a, b, sems.at[at]) for at, (a, b) in enumerate(zip(sources, targets))]
    for copy in copies:
        copy.start()
    for copy in copies:
        copy.wait()


def body(late_input, up_weight, down_weight, early_input, early_pre, cotangent, up_sum, down_sum):
    vmem = pl.BlockSpec(memory_space=pltpu.VMEM)
    anywhere = pl.BlockSpec(memory_space=pl.ANY)
    dma = pltpu.SemaphoreType.DMA
    results = (((128, 4096), BF16), ((128, 256), BF16), ((128, 256), BF16), ((64, 256), F32), ((64, 256), F32))
    held = pl.pallas_call(
        kernel,
        out_shape=tuple(pltpu.VMEM(shape, dtype) for shape, dtype in results),
        in_specs=[anywhere] * 8,
        out_specs=(vmem,) * 5,
        scratch_shapes=[
            pltpu.VMEM((128, 256), BF16),
            pltpu.VMEM((64, 256), BF16),
            pltpu.VMEM((64, 256), BF16),
            pltpu.VMEM((128, 256), BF16),
            pltpu.VMEM((128, 4096), BF16),
            pltpu.VMEM((128, 256), BF16),
            pltpu.VMEM((64, 256), F32),
            pltpu.VMEM((64, 256), F32),
            pltpu.VMEM((2, 2, 8, 8, 32, 256), BF16),
            pltpu.VMEM((2, 2, 8, 8, 32, 256), BF16),
            pltpu.VMEM((2, 2, 2, 4, 8, 32, 256), BF16),
            pltpu.VMEM((2, 2, 7, 32, 256), BF16),
            pltpu.VMEM((2, 8, 8, 32, 128), BF16),
            pltpu.VMEM((256, 128), BF16),
            pltpu.VMEM((256, 128), BF16),
            pltpu.VMEM((2, 4, 1024, 128), BF16),
            pltpu.VMEM((2, 4, 512, 128), BF16),
            pltpu.VMEM((2, 4, 512, 128), BF16),
            pltpu.VMEM((2, 4, 3, 128, 128), BF16),
            pltpu.VMEM((2, 2, 8, 8, 32, 128), BF16),
            pltpu.VMEM((2, 128, 256), F32),
            dma((8,)), dma((2, 2)),
            dma((2,)), dma((5,)),
            dma((2, 2)), dma((2, 2, 4, 2)),
            dma((2, 2)), dma((2, 2, 4, 2)),
            dma((2,)), dma((5,)),
            dma((2, 4)), dma((2, 4)), dma((2, 4)), dma((2, 4)), dma((2, 4)),
        ],
        compiler_params=pltpu.CompilerParams(
            collective_id=0, has_side_effects=True, vmem_limit_bytes=36 * 1024 * 1024
        ),
        cost_estimate=pl.CostEstimate(flops=1_700_000_000, bytes_accessed=8_000_000, transcendentals=0),
    )(*(
        pltpu.with_memory_space_constraint(value, pltpu.MemorySpace.HBM)
        for value in (
            late_input, up_weight.T, down_weight, early_input, early_pre, cotangent, up_sum.T, down_sum
        )
    ))
    outs = pl.pallas_call(
        deliver,
        out_shape=tuple(jax.ShapeDtypeStruct(shape, dtype) for shape, dtype in results),
        in_specs=[vmem] * 5,
        out_specs=(anywhere,) * 5,
        scratch_shapes=[dma((5,))],
        compiler_params=pltpu.CompilerParams(vmem_limit_bytes=8 * 1024 * 1024),
    )(*held)
    late_pre, late_out, input_grad, up_total, down_total = outs
    return late_pre, late_out, input_grad, up_total.T, down_total


def solution(mesh):
    split = Mesh(mesh.devices.reshape(8, 8, 4, 2), FS + TP)
    placed = (
        P(FS, TP), P(TP, FS), P(FS, TP), P(FS, TP), P(FS, None), P(FS, TP), P(TP, FS), P(FS, TP),
    )
    return jax.shard_map(
        body,
        mesh=split,
        in_specs=placed,
        out_specs=(P(FS, None), P(FS, TP), P(FS, TP), P(TP, FS), P(FS, TP)),
        check_vma=False,
    )
```

```python
import jax
import jax.numpy as jnp
from jax import lax
from jax.experimental import pallas as pl
from jax.experimental.pallas import tpu as pltpu
from jax.sharding import Mesh
from jax.sharding import PartitionSpec as P

FS = ("z", "y")
TP = ("x", "c")
MESH = pl.DeviceIdType.MESH
F32 = jnp.float32
BF16 = jnp.bfloat16
BLOCK_AXIS = ("z", "y")
SUB_AXIS = ("y", "z")
GATHER_PARTS = (4, 4)
SCATTER_PARTS = (4, 4)


def nn(left, right):
    return lax.dot_general(left, right, (((1,), (0,)), ((), ())), preferred_element_type=F32)


def tn(left, right):
    return lax.dot_general(left, right, (((0,), (0,)), ((), ())), preferred_element_type=F32)


def square_relu(value):
    return jnp.square(jnp.maximum(value.astype(F32), 0.0)).astype(BF16)


def kernel(
    late_in_h, up_t_h, down_h, early_in_h, early_pre_h, cot_h, up_sum_h, down_sum_h,
    late_pre_o, late_out_o, input_grad_o, up_total_o, down_total_o,
    late_in, up_t, down, early_in, early_pre, cot, up_sum, down_sum,
    weights, grads, ring_in, last_in, early_t, cot_t, late_t, part, pair_in, pair_sum, x_in, full, acc,
    in_sem, own_sem, ag1_s, ag1_r, ag2_s, ag2_r, rs1_s, rs1_r, rs2_s, rs2_r,
    tp_s, pair_r, xr_r, xg_r, fw_r,
):
    iz, iy, ix, ic = (lax.axis_index(name) for name in ("z", "y", "x", "c"))
    place = (iz, iy)
    sub_place = (iy, iz)
    shards = (down, up_t)

    def up_by(value, step, size=8):
        return lax.rem(value + (step % size), size)

    def send(src, dst, send_sem, recv_sem, axis, index):
        pltpu.make_async_remote_copy(
            src_ref=src, dst_ref=dst, send_sem=send_sem, recv_sem=recv_sem,
            device_id={axis: index}, device_id_type=MESH,
        ).start()

    def arrive(ref, recv_sem):
        pltpu.make_async_remote_copy(
            src_ref=ref, dst_ref=ref, send_sem=recv_sem, recv_sem=recv_sem,
            device_id={"c": up_by(ic, 1, 2)}, device_id_type=MESH,
        ).wait_recv()

    def gone(ref, send_sem):
        pltpu.make_async_remote_copy(
            src_ref=ref, dst_ref=ref, send_sem=send_sem, recv_sem=send_sem,
            device_id={"c": up_by(ic, 1, 2)}, device_id_type=MESH,
        ).wait_send()

    barrier = pltpu.get_barrier_semaphore()
    for axis, me, size in (("y", iy, 8), ("z", iz, 8), ("x", ix, 4), ("c", ic, 2)):
        for step in range(1, size):
            pl.semaphore_signal(
                barrier, inc=1, device_id={axis: up_by(me, step, size)}, device_id_type=MESH
            )
    loads = []
    for at, (source, target) in enumerate((
        (down_h, down), (up_t_h, up_t), (cot_h, cot), (late_in_h, late_in), (early_pre_h, early_pre),
        (early_in_h, early_in), (down_sum_h, down_sum), (up_sum_h, up_sum),
    )):
        copy = pltpu.make_async_copy(source, target, in_sem.at[at])
        copy.start()
        loads.append(copy)
    def slot(sub, h):
        return lax.rem(sub - sub_place[h] + 9, 8)

    def early(quarter):
        def one(at, _):
            z, y = at // 4, 2 * lax.rem(at, 4)
            turned = early_pre[:, pl.ds(pl.multiple_of(at * 128, 128), 128)].T
            early_t[0, z, slot(y, 0)] = turned[0:32]
            early_t[1, y, slot(z, 1)] = turned[32:64]
            early_t[0, z, slot(y + 1, 0)] = turned[64:96]
            early_t[1, y + 1, slot(z, 1)] = turned[96:128]
            return 0

        lax.fori_loop(8 * quarter, 8 * quarter + 8, one, 0)

    loads[2].wait()
    cot_t[...] = cot[...].T
    loads[4].wait()
    early(0)
    early(1)
    early(2)
    loads[0].wait()
    pl.semaphore_wait(barrier, 18)

    own = []

    def own_copy(w):
        if w == 1:
            loads[1].wait()
        for h in range(2):
            rows = shards[w].at[pl.ds(32 * h, 32), :]
            copy = pltpu.make_async_copy(rows, weights.at[w, h, place[h], 1], own_sem.at[w, h])
            copy.start()
            own.append(copy)

    def others_in(part_at, parts):
        slots = range(part_at * 8 // parts, (part_at + 1) * 8 // parts)
        return [at for at in slots if at != 1]

    def ag1_send(w):
        for part_at in range(GATHER_PARTS[w]):
            for at in others_in(part_at, GATHER_PARTS[w])[::-1]:
                for h in range(2):
                    send(
                        shards[w].at[pl.ds(32 * h, 32), :], weights.at[w, h, place[h], at],
                        ag1_s.at[w], ag1_r.at[5 + part_at], SUB_AXIS[h], up_by(sub_place[h], 1 - at),
                    )

    def ag1_wait(w, part_at):
        if part_at == 0:
            for h in range(2):
                own[2 * w + h].wait()
        count = len(others_in(part_at, GATHER_PARTS[w]))
        arrive(weights.at[w, 0, pl.ds(0, 2), pl.ds(0, count)], ag1_r.at[5 + part_at])

    def ring_send(w, h, way, step):
        sign = (1 - 2 * way) * (1 - 2 * h)
        ref = weights.at[w, h, place[h], (9 - sign * (step - 1)) % 8]
        target = weights.at[w, h, place[h], (9 - sign * step) % 8]
        send(ref, target, ag1_s.at[w], ag1_r.at[step], SUB_AXIS[h], up_by(sub_place[h], sign))

    def ag1_ring_start(w):
        for h in range(2):
            own[2 * w + h].wait()
            for way in range(2):
                ring_send(w, h, way, 1)

    def ag1_ring_step(w, step):
        arrive(weights.at[w, 0, 0, pl.ds(0, 4 if step < 4 else 2)], ag1_r.at[step])
        for h in range(2):
            for way in range(2):
                if step + way < 4:
                    ring_send(w, h, way, step + 1)

    def ag2_send(w, h, way, step, part_at):
        sign = 1 - 2 * way
        size = 8 // GATHER_PARTS[w]
        ref = weights.at[w, h, up_by(place[h], -sign * (step - 1)), pl.ds(size * part_at, size)]
        send(ref, ref, ag2_s.at[w, h], ag2_r.at[w, h, step - 1, part_at], BLOCK_AXIS[h], up_by(place[h], sign))

    def ag2_start(w, part_at):
        for h in range(2):
            for way in range(2):
                ag2_send(w, h, way, 1, part_at)

    def ag2_part(w, step, part_at):
        parts = GATHER_PARTS[w]
        size = (16 if step < 4 else 8) // parts
        for h in range(2):
            arrive(weights.at[w, h, 0, pl.ds(0, size)], ag2_r.at[w, h, step - 1, part_at])
            for way in range(2):
                if step < 3 or (step == 3 and 2 * part_at // parts == way):
                    ag2_send(w, h, way, step + 1, part_at)

    def rs_send(w, h, way, step, part_at):
        sign = 1 - 2 * way
        size = 8 // SCATTER_PARTS[w]
        send(
            grads.at[w, h, up_by(place[h], sign * (5 - step)), pl.ds(size * part_at, size)],
            ring_in.at[w, h, way, step - 1, pl.ds(size * part_at, size)],
            rs1_s.at[w, h], rs1_r.at[w, h, step - 1, part_at], BLOCK_AXIS[h], up_by(place[h], sign),
        )

    def rs_start(w):
        parts = SCATTER_PARTS[w]
        for step in (1, 2):
            for part_at in ((1, 0), (2, 3, 1, 0))[parts // 4]:
                way = (2 * part_at // parts + step - 1) % 2
                for h in range(2):
                    rs_send(w, h, way, step, part_at)

    def rs_part(w, step, part_at):
        parts = SCATTER_PARTS[w]
        size = 8 // parts
        for h in range(2):
            arrive(weights.at[w, h, 0, pl.ds(0, 2 * size if step > 1 else size)], rs1_r.at[w, h, step - 1, part_at])
            for way in range(2):
                if step == 1 and 2 * part_at // parts != way:
                    continue
                arrived = ring_in.at[w, h, way, step - 1, pl.ds(size * part_at, size)]
                block = up_by(place[h], (1 - 2 * way) * (4 - step))
                mine = grads.at[w, h, block, pl.ds(size * part_at, size)]
                mine[...] = (mine[...].astype(F32) + arrived[...].astype(F32)).astype(BF16)
                rs_send(w, h, way, step + 1, part_at)

    def rs_last(w, part_at):
        size = 8 // SCATTER_PARTS[w]
        for h in range(2):
            arrive(weights.at[w, h, 0, pl.ds(0, 2 * size)], rs1_r.at[w, h, 3, part_at])
            mine = grads.at[w, h, place[h], pl.ds(size * part_at, size)]
            total = mine[...].astype(F32)
            for way in range(2):
                total = total + ring_in[w, h, way, 3, pl.ds(size * part_at, size)].astype(F32)
            mine[...] = total.astype(BF16)

    def rs2_send(w, part_at):
        for at in others_in(part_at, SCATTER_PARTS[w])[::-1]:
            for h in range(2):
                send(
                    grads.at[w, h, place[h], at], last_in.at[w, h, (at - 2) % 8],
                    rs2_s.at[w], rs2_r.at[5 + part_at], SUB_AXIS[h], up_by(sub_place[h], at - 1),
                )

    def rs2_ring_send(w, h, way, step):
        sign = (1 - 2 * way) * (1 - 2 * h)
        send(
            grads.at[w, h, place[h], (sign * (5 - way - step) + 1) % 8],
            last_in.at[w, h, 4 * way + step - 1],
            rs2_s.at[w], rs2_r.at[step], SUB_AXIS[h], up_by(sub_place[h], sign),
        )

    def rs2_ring_start(w):
        for h in range(2):
            for way in range(2):
                rs2_ring_send(w, h, way, 1)

    def rs2_ring_step(w, step):
        arrive(weights.at[w, 0, 0, pl.ds(0, 4)], rs2_r.at[step])
        for h in range(2):
            for way in range(2):
                if step + way < 4:
                    sign = (1 - 2 * way) * (1 - 2 * h)
                    mine = grads.at[w, h, place[h], (sign * (4 - way - step) + 1) % 8]
                    arrived = last_in[w, h, 4 * way + step - 1]
                    mine[...] = (mine[...].astype(F32) + arrived.astype(F32)).astype(BF16)
                    rs2_ring_send(w, h, way, step + 1)

    def rs_out(w, ring):
        base, out = ((down_sum, down_total_o), (up_sum, up_total_o))[w]
        if ring:
            arrive(weights.at[w, 0, 0, pl.ds(0, 2)], rs2_r.at[4])
        else:
            for part_at in range(SCATTER_PARTS[w]):
                count = len(others_in(part_at, SCATTER_PARTS[w]))
                arrive(weights.at[w, 0, pl.ds(0, 2), pl.ds(0, count)], rs2_r.at[5 + part_at])
        for h in range(2):
            total = grads[w, h, place[h], 1].astype(F32)
            for at in (3, 6) if ring else range(7):
                total = total + last_in[w, h, at].astype(F32)
            rows = pl.ds(32 * h, 32)
            out[rows, :] = base[rows, :] + total

    def block_of(h, side, j):
        return lax.rem(iz * (1 - h) + iy * h + side * (2 * j + 1) - j + 8, 8)

    def product(a, j, sides):
        w, right = ((0, cot_t), (1, late_t))[a]

        def one(h, _):
            for side in sides:
                rows = weights[w, h, block_of(h, side, j)].reshape(256, 256)
                part[a, j, pl.ds(pl.multiple_of(h * 512 + side * 256, 256), 256), :] = nn(
                    rows, right[...]
                ).astype(BF16)
            return 0

        lax.fori_loop(0, 2, one, 0)

    other = up_by(ic, 1, 2)
    my_half = pl.multiple_of(ic * 512, 512)
    other_half = pl.multiple_of(other * 512, 512)

    def s1(a, j):
        send(
            part.at[a, j, pl.ds(other_half, 512), :], pair_in.at[a, j],
            tp_s.at[a, 0], pair_r.at[a, j], "c", other,
        )

    def s2(a, j):
        arrive(pair_in.at[a, j], pair_r.at[a, j])
        pair_sum[a, j] = (
            part[a, j, pl.ds(my_half, 512), :].astype(F32) + pair_in[a, j].astype(F32)
        ).astype(BF16)
        for step in (2, 1, 3):
            target = up_by(ix, step, 4)
            rows = pl.ds(pl.multiple_of(target * 128, 128), 128)
            send(pair_sum.at[a, j, rows, :], x_in.at[a, j, step - 1], tp_s.at[a, 1], xr_r.at[a, j], "x", target)

    def share(a, core, x, j):
        return full.at[a, core, block_of(core, x // 2, j), pl.ds(4 * lax.rem(x, 2), 4)]

    def s3(a, j):
        total = pair_sum[a, j, pl.ds(pl.multiple_of(ix * 128, 128), 128), :].astype(F32)
        arrive(x_in.at[a, j], xr_r.at[a, j])
        for at in range(3):
            total = total + x_in[a, j, at].astype(F32)
        if a == 0:
            block = block_of(ic, ix // 2, j)
            saved = early_t[ic, block, pl.ds(4 * lax.rem(ix, 2), 4)].reshape(128, 128)
            total = total * 2.0 * jnp.maximum(saved.astype(F32), 0.0)
        ref = share(a, ic, ix, j)
        ref[...] = total.astype(BF16).reshape(4, 32, 128)
        for step in (2, 1, 3):
            send(ref, ref, tp_s.at[a, 2], xg_r.at[a, j], "x", up_by(ix, step, 4))
        send(ref, ref, tp_s.at[a, 3], fw_r.at[a, j], "c", other)

    def s4(a, j):
        arrive(x_in.at[a, j], xg_r.at[a, j])
        for step in (1, 2, 3):
            ref = share(a, ic, up_by(ix, step, 4), j)
            send(ref, ref, tp_s.at[a, 3], fw_r.at[a, j], "c", other)

    def s5(a, j):
        arrive(pair_in.at[a, j], fw_r.at[a, j])

    def all_gone():
        small = weights.at[0, 0, pl.ds(0, 7), pl.ds(0, 2)]
        for w in range(2):
            gone(small, ag1_s.at[w])
            gone(small, rs2_s.at[w])
            for h in range(2):
                gone(weights.at[w, h, pl.ds(0, 7)], ag2_s.at[w, h])
                gone(weights.at[w, h, pl.ds(0, 7)], rs1_s.at[w, h])
            gone(pair_in.at[w], tp_s.at[w, 0])
            gone(x_in.at[w], tp_s.at[w, 1])
            gone(x_in.at[w], tp_s.at[w, 2])
            gone(pair_in.at[w], tp_s.at[w, 3])

    def pieces(j, fn):
        def one(at, _):
            h, side = at // 2, lax.rem(at, 2)
            fn(h, block_of(h, side, j))
            return 0

        lax.fori_loop(0, 4, one, 0)

    def up_grads(j):
        def fn(h, block):
            rows = full[0, h, block].reshape(256, 128)
            grads[1, h, block] = nn(rows, early_in[...]).astype(BF16).reshape(8, 32, 256)

        pieces(j, fn)

    def input_grads(j):
        def fn(h, block):
            acc[0] += tn(full[0, h, block].reshape(256, 128), weights[1, h, block].reshape(256, 256))

        pieces(j, fn)

    def late_outs(j):
        def fn(h, block):
            hidden = square_relu(full[1, h, block].reshape(256, 128))
            acc[1] += tn(hidden, weights[0, h, block].reshape(256, 256))

        pieces(j, fn)

    def turn_late(quarter):
        def one(at, _):
            z, y = at // 4, 2 * lax.rem(at, 4)
            rows = jnp.concatenate(
                [
                    full[1, 0, z, slot(y, 0)], full[1, 1, y, slot(z, 1)],
                    full[1, 0, z, slot(y + 1, 0)], full[1, 1, y + 1, slot(z, 1)],
                ],
                axis=0,
            )
            late_pre_o[:, pl.ds(pl.multiple_of(at * 128, 128), 128)] = rows.T
            return 0

        lax.fori_loop(8 * quarter, 8 * quarter + 8, one, 0)

    def down_grads(j):
        def fn(h, block):
            hidden = square_relu(early_t[h, block].reshape(256, 128))
            grads[0, h, block] = nn(hidden, cot[...]).astype(BF16).reshape(8, 32, 256)

        pieces(j, fn)

    def prep_late():
        loads[3].wait()
        late_t[...] = late_in[...].T
        acc[...] = jnp.zeros_like(acc)
        loads[5].wait()
        loads[6].wait()
        loads[7].wait()

    def fin_late():
        late_out_o[...] = acc[1].astype(BF16)

    def fin_input():
        input_grad_o[...] = acc[0].astype(BF16)

    own_copy(0)
    ag1_send(0)
    early(3)
    down_grads(2)
    down_grads(0)
    own_copy(1)
    prep_late()
    down_grads(1)
    down_grads(3)
    ag1_wait(0, 0)
    ag1_wait(0, 1)
    ag2_start(0, 0)
    ag2_start(0, 1)
    ag1_ring_start(1)
    ag1_wait(0, 2)
    ag2_start(0, 2)
    ag1_wait(0, 3)
    ag2_start(0, 3)
    product(0, 0, (0,))
    ag2_part(0, 1, 0)
    ag1_ring_step(1, 1)
    ag2_start(1, 0)
    ag2_part(0, 1, 2)
    ag2_part(0, 1, 1)
    ag2_part(0, 1, 3)
    product(0, 0, (1,))
    product(0, 1, (0,))
    ag2_part(0, 2, 0)
    s1(0, 0)
    ag1_ring_step(1, 2)
    ag2_start(1, 1)
    ag2_part(1, 1, 0)
    s2(0, 0)
    ag2_part(0, 2, 2)
    ag2_part(0, 2, 1)
    ag2_part(0, 2, 3)
    product(0, 1, (1,))
    s1(0, 1)
    product(0, 2, (0,))
    ag2_part(0, 3, 0)
    ag1_ring_step(1, 3)
    s2(0, 1)
    ag2_part(1, 2, 0)
    ag2_start(1, 3)
    s3(0, 0)
    ag2_part(0, 3, 2)
    ag2_part(0, 3, 1)
    ag2_part(0, 3, 3)
    product(0, 2, (1,))
    s1(0, 2)
    ag2_part(1, 1, 1)
    product(0, 3, (0,))
    ag2_part(0, 4, 0)
    ag1_ring_step(1, 4)
    ag2_start(1, 2)
    product(1, 0, (0,))
    ag2_part(1, 3, 0)
    s2(0, 2)
    s3(0, 1)
    ag2_part(1, 1, 3)
    ag2_part(0, 4, 2)
    ag2_part(0, 4, 1)
    rs_start(0)
    ag2_part(0, 4, 3)
    product(0, 3, (1,))
    s1(0, 3)
    ag2_part(1, 2, 1)
    s4(0, 0)
    ag2_part(1, 1, 2)
    product(1, 0, (1,))
    s1(1, 0)
    s2(0, 3)
    product(1, 1, (0,))
    ag2_part(1, 4, 0)
    s5(0, 0)
    up_grads(0)
    ag2_part(1, 2, 3)
    s3(0, 2)
    rs_part(0, 1, 2)
    rs_part(0, 1, 0)
    rs_part(0, 1, 3)
    rs_part(0, 1, 1)
    s4(0, 1)
    ag2_part(1, 3, 1)
    s5(0, 1)
    up_grads(1)
    ag2_part(1, 2, 2)
    s3(0, 3)
    product(1, 1, (1,))
    ag2_part(1, 3, 3)
    s1(1, 1)
    product(1, 2, (0,))
    rs_part(0, 2, 2)
    rs_part(0, 2, 3)
    rs_part(0, 2, 1)
    s2(1, 1)
    s4(0, 2)
    ag2_part(1, 4, 1)
    rs_part(0, 2, 0)
    ag2_part(1, 3, 2)
    product(1, 2, (1,))
    product(1, 3, (0,))
    s5(0, 2)
    up_grads(2)
    rs_part(0, 3, 2)
    s1(1, 2)
    ag2_part(1, 4, 3)
    s2(1, 0)
    s4(0, 3)
    rs_part(0, 3, 3)
    s2(1, 2)
    rs_part(0, 3, 1)
    s5(0, 3)
    up_grads(3)
    rs_start(1)
    rs_part(0, 3, 0)
    s3(1, 1)
    ag2_part(1, 4, 2)
    product(1, 3, (1,))
    input_grads(3)
    s1(1, 3)
    input_grads(0)
    rs_last(0, 2)
    input_grads(2)
    rs_last(0, 1)
    rs_part(1, 1, 2)
    s2(1, 3)
    rs_last(0, 3)
    input_grads(1)
    fin_input()
    rs_part(1, 1, 3)
    rs_part(1, 1, 0)
    s3(1, 0)
    s3(1, 2)
    rs_part(1, 1, 1)
    rs_last(0, 0)
    rs2_ring_start(0)
    rs_part(1, 2, 2)
    s4(1, 1)
    rs_part(1, 2, 3)
    rs_part(1, 2, 0)
    rs_part(1, 2, 1)
    s5(1, 1)
    late_outs(1)
    s3(1, 3)
    rs2_ring_step(0, 1)
    rs_part(1, 3, 2)
    s4(1, 0)
    rs_part(1, 3, 3)
    rs_part(1, 3, 0)
    rs_part(1, 3, 1)
    s5(1, 0)
    late_outs(0)
    rs2_ring_step(0, 2)
    s4(1, 2)
    rs_last(1, 2)
    rs2_send(1, 2)
    rs_last(1, 3)
    rs2_send(1, 3)
    s5(1, 2)
    late_outs(2)
    rs_last(1, 0)
    rs2_send(1, 0)
    s4(1, 3)
    rs_last(1, 1)
    rs2_send(1, 1)
    rs2_ring_step(0, 3)
    s5(1, 3)
    late_outs(3)
    fin_late()
    turn_late(0)
    turn_late(1)
    turn_late(3)
    turn_late(2)
    rs_out(0, True)
    rs_out(1, False)
    all_gone()


def deliver(*refs):
    sources, targets, sems = refs[:5], refs[5:10], refs[10]
    copies = [pltpu.make_async_copy(a, b, sems.at[at]) for at, (a, b) in enumerate(zip(sources, targets))]
    for copy in copies:
        copy.start()
    for copy in copies:
        copy.wait()


def body(late_input, up_weight, down_weight, early_input, early_pre, cotangent, up_sum, down_sum):
    vmem = pl.BlockSpec(memory_space=pltpu.VMEM)
    anywhere = pl.BlockSpec(memory_space=pl.ANY)
    dma = pltpu.SemaphoreType.DMA
    results = (((128, 4096), BF16), ((128, 256), BF16), ((128, 256), BF16), ((64, 256), F32), ((64, 256), F32))
    held = pl.pallas_call(
        kernel,
        out_shape=tuple(pltpu.VMEM(shape, dtype) for shape, dtype in results),
        in_specs=[anywhere] * 8,
        out_specs=(vmem,) * 5,
        scratch_shapes=[
            pltpu.VMEM((128, 256), BF16),
            pltpu.VMEM((64, 256), BF16),
            pltpu.VMEM((64, 256), BF16),
            pltpu.VMEM((128, 256), BF16),
            pltpu.VMEM((128, 4096), BF16),
            pltpu.VMEM((128, 256), BF16),
            pltpu.VMEM((64, 256), F32),
            pltpu.VMEM((64, 256), F32),
            pltpu.VMEM((2, 2, 8, 8, 32, 256), BF16),
            pltpu.VMEM((2, 2, 8, 8, 32, 256), BF16),
            pltpu.VMEM((2, 2, 2, 4, 8, 32, 256), BF16),
            pltpu.VMEM((2, 2, 7, 32, 256), BF16),
            pltpu.VMEM((2, 8, 8, 32, 128), BF16),
            pltpu.VMEM((256, 128), BF16),
            pltpu.VMEM((256, 128), BF16),
            pltpu.VMEM((2, 4, 1024, 128), BF16),
            pltpu.VMEM((2, 4, 512, 128), BF16),
            pltpu.VMEM((2, 4, 512, 128), BF16),
            pltpu.VMEM((2, 4, 3, 128, 128), BF16),
            pltpu.VMEM((2, 2, 8, 8, 32, 128), BF16),
            pltpu.VMEM((2, 128, 256), F32),
            dma((8,)), dma((2, 2)),
            dma((2,)), dma((9,)),
            dma((2, 2)), dma((2, 2, 4, 4)),
            dma((2, 2)), dma((2, 2, 4, 4)),
            dma((2,)), dma((9,)),
            dma((2, 4)), dma((2, 4)), dma((2, 4)), dma((2, 4)), dma((2, 4)),
        ],
        compiler_params=pltpu.CompilerParams(
            collective_id=0, has_side_effects=True, vmem_limit_bytes=36 * 1024 * 1024
        ),
        cost_estimate=pl.CostEstimate(flops=1_700_000_000, bytes_accessed=8_000_000, transcendentals=0),
    )(*(
        pltpu.with_memory_space_constraint(value, pltpu.MemorySpace.HBM)
        for value in (
            late_input, up_weight.T, down_weight, early_input, early_pre, cotangent, up_sum.T, down_sum
        )
    ))
    outs = pl.pallas_call(
        deliver,
        out_shape=tuple(jax.ShapeDtypeStruct(shape, dtype) for shape, dtype in results),
        in_specs=[vmem] * 5,
        out_specs=(anywhere,) * 5,
        scratch_shapes=[dma((5,))],
        compiler_params=pltpu.CompilerParams(vmem_limit_bytes=8 * 1024 * 1024),
    )(*held)
    late_pre, late_out, input_grad, up_total, down_total = outs
    return late_pre, late_out, input_grad, up_total.T, down_total


def solution(mesh):
    split = Mesh(mesh.devices.reshape(8, 8, 4, 2), FS + TP)
    placed = (
        P(FS, TP), P(TP, FS), P(FS, TP), P(FS, TP), P(FS, None), P(FS, TP), P(TP, FS), P(FS, TP),
    )
    return jax.shard_map(
        body,
        mesh=split,
        in_specs=placed,
        out_specs=(P(FS, None), P(FS, TP), P(FS, TP), P(TP, FS), P(FS, TP)),
        check_vma=False,
    )
```

```python
import jax
import jax.numpy as jnp
from jax import lax
from jax.experimental import pallas as pl
from jax.experimental.pallas import tpu as pltpu
from jax.sharding import Mesh
from jax.sharding import PartitionSpec as P

FS = ("z", "y")
TP = ("x", "c")
MESH = pl.DeviceIdType.MESH
F32 = jnp.float32
BF16 = jnp.bfloat16
BLOCK_AXIS = ("z", "y")
SUB_AXIS = ("y", "z")
GATHER_PARTS = (4, 4)
SCATTER_PARTS = (4, 4)


def nn(left, right):
    return lax.dot_general(left, right, (((1,), (0,)), ((), ())), preferred_element_type=F32)


def tn(left, right):
    return lax.dot_general(left, right, (((0,), (0,)), ((), ())), preferred_element_type=F32)


def square_relu(value):
    return jnp.square(jnp.maximum(value.astype(F32), 0.0)).astype(BF16)


def kernel(
    late_in_h, up_t_h, down_h, early_in_h, early_pre_h, cot_h, up_sum_h, down_sum_h,
    late_pre_o, late_out_o, input_grad_o, up_total_o, down_total_o,
    late_in, up_t, down, early_in, early_pre, cot, up_sum, down_sum,
    weights, grads, ring_in, last_in, early_t, cot_t, late_t, part, pair_in, pair_sum, x_in, full, acc,
    in_sem, own_sem, ag1_s, ag1_r, ag2_s, ag2_r, rs1_s, rs1_r, rs2_s, rs2_r,
    tp_s, pair_r, xr_r, xg_r, fw_r,
):
    iz, iy, ix, ic = (lax.axis_index(name) for name in ("z", "y", "x", "c"))
    place = (iz, iy)
    sub_place = (iy, iz)
    shards = (down, up_t)

    def up_by(value, step, size=8):
        return lax.rem(value + (step % size), size)

    def send(src, dst, send_sem, recv_sem, axis, index):
        pltpu.make_async_remote_copy(
            src_ref=src, dst_ref=dst, send_sem=send_sem, recv_sem=recv_sem,
            device_id={axis: index}, device_id_type=MESH,
        ).start()

    def arrive(ref, recv_sem):
        pltpu.make_async_remote_copy(
            src_ref=ref, dst_ref=ref, send_sem=recv_sem, recv_sem=recv_sem,
            device_id={"c": up_by(ic, 1, 2)}, device_id_type=MESH,
        ).wait_recv()

    def gone(ref, send_sem):
        pltpu.make_async_remote_copy(
            src_ref=ref, dst_ref=ref, send_sem=send_sem, recv_sem=send_sem,
            device_id={"c": up_by(ic, 1, 2)}, device_id_type=MESH,
        ).wait_send()

    barrier = pltpu.get_barrier_semaphore()
    steps = [(step, axis, me, 8) for step in (4, 5, 3, 6, 2, 7, 1) for axis, me in (("z", iz), ("y", iy))]
    steps += [(step, "x", ix, 4) for step in (2, 1, 3)] + [(1, "c", ic, 2)]
    for step, axis, me, size in steps:
        pl.semaphore_signal(
            barrier, inc=1, device_id={axis: up_by(me, step, size)}, device_id_type=MESH
        )
    loads = []
    for at, source, target in (
        (0, down_h, down), (1, cot_h, cot), (2, early_pre_h, early_pre), (3, up_t_h, up_t), (3, late_in_h, late_in),
        (3, early_in_h, early_in), (3, down_sum_h, down_sum), (3, up_sum_h, up_sum),
    ):
        copy = pltpu.make_async_copy(source, target, in_sem.at[at])
        copy.start()
        loads.append(copy)
    def slot(sub, h):
        return lax.rem(sub - sub_place[h] + 9, 8)

    def early(quarter):
        def one(at, _):
            z, y = at // 4, 2 * lax.rem(at, 4)
            turned = early_pre[:, pl.ds(pl.multiple_of(at * 128, 128), 128)].T
            early_t[0, z, slot(y, 0)] = turned[0:32]
            early_t[1, y, slot(z, 1)] = turned[32:64]
            early_t[0, z, slot(y + 1, 0)] = turned[64:96]
            early_t[1, y + 1, slot(z, 1)] = turned[96:128]
            return 0

        lax.fori_loop(8 * quarter, 8 * quarter + 8, one, 0)

    loads[1].wait()
    cot_t[...] = cot[...].T
    loads[2].wait()
    early(0)
    early(1)
    early(2)
    loads[0].wait()
    pl.semaphore_wait(barrier, 18)

    def own_copy(w):
        if w == 1:
            rest = weights.at[:, 1, pl.ds(0, 3), pl.ds(0, 3)]
            pltpu.make_async_copy(rest, rest, in_sem.at[3]).wait()
        for h in range(2):
            rows = shards[w].at[pl.ds(32 * h, 32), :]
            pltpu.make_async_copy(rows, weights.at[w, h, place[h], 1], own_sem.at[w]).start()

    def own_wait(w):
        both = weights.at[w, :, 0, 0]
        pltpu.make_async_copy(both, both, own_sem.at[w]).wait()

    def others_in(part_at, parts):
        slots = range(part_at * 8 // parts, (part_at + 1) * 8 // parts)
        return [at for at in slots if at != 1]

    def ag1_send(w):
        for part_at in range(GATHER_PARTS[w]):
            for at in others_in(part_at, GATHER_PARTS[w])[::-1]:
                for h in range(2):
                    send(
                        shards[w].at[pl.ds(32 * h, 32), :], weights.at[w, h, place[h], at],
                        ag1_s.at[w], ag1_r.at[5 + part_at], SUB_AXIS[h], up_by(sub_place[h], 1 - at),
                    )

    def ag1_wait(w, part_at):
        if part_at == 0:
            own_wait(w)
        count = len(others_in(part_at, GATHER_PARTS[w]))
        arrive(weights.at[w, 0, pl.ds(0, 2), pl.ds(0, count)], ag1_r.at[5 + part_at])

    def ring_send(w, h, way, step):
        sign = (1 - 2 * way) * (1 - 2 * h)
        ref = weights.at[w, h, place[h], (9 - sign * (step - 1)) % 8]
        target = weights.at[w, h, place[h], (9 - sign * step) % 8]
        send(ref, target, ag1_s.at[w], ag1_r.at[step], SUB_AXIS[h], up_by(sub_place[h], sign))

    def ag1_ring_start(w):
        own_wait(w)
        for h in range(2):
            for way in range(2):
                ring_send(w, h, way, 1)

    def ag1_ring_step(w, step):
        arrive(weights.at[w, 0, 0, pl.ds(0, 4 if step < 4 else 2)], ag1_r.at[step])
        for h in range(2):
            for way in range(2):
                if step + way < 4:
                    ring_send(w, h, way, step + 1)

    def ag2_send(w, h, way, step, part_at):
        sign = 1 - 2 * way
        size = 8 // GATHER_PARTS[w]
        ref = weights.at[w, h, up_by(place[h], -sign * (step - 1)), pl.ds(size * part_at, size)]
        send(ref, ref, ag2_s.at[w], ag2_r.at[w, step - 1, part_at], BLOCK_AXIS[h], up_by(place[h], sign))

    def ag2_start(w, part_at):
        for h in range(2):
            for way in range(2):
                ag2_send(w, h, way, 1, part_at)

    def ag2_part(w, step, part_at):
        parts = GATHER_PARTS[w]
        size = (16 if step < 4 else 8) // parts
        arrive(weights.at[w, :, 0, pl.ds(0, size)], ag2_r.at[w, step - 1, part_at])
        for h in range(2):
            for way in range(2):
                if step < 3 or (step == 3 and 2 * part_at // parts == way):
                    ag2_send(w, h, way, step + 1, part_at)

    def rs_send(w, h, way, step, part_at):
        sign = 1 - 2 * way
        size = 8 // SCATTER_PARTS[w]
        send(
            grads.at[w, h, up_by(place[h], sign * (5 - step)), pl.ds(size * part_at, size)],
            ring_in.at[w, h, way, step - 1, pl.ds(size * part_at, size)],
            rs1_s.at[w], rs1_r.at[w, step - 1, part_at], BLOCK_AXIS[h], up_by(place[h], sign),
        )

    def rs_start(w):
        parts = SCATTER_PARTS[w]
        for step in (1, 2):
            for part_at in ((1, 0), (2, 3, 1, 0))[parts // 4]:
                way = (2 * part_at // parts + step - 1) % 2
                for h in range(2):
                    rs_send(w, h, way, step, part_at)

    def rs_part(w, step, part_at):
        parts = SCATTER_PARTS[w]
        size = 8 // parts
        arrive(weights.at[w, :, 0, pl.ds(0, 2 * size if step > 1 else size)], rs1_r.at[w, step - 1, part_at])
        for h in range(2):
            for way in range(2):
                if step == 1 and 2 * part_at // parts != way:
                    continue
                arrived = ring_in.at[w, h, way, step - 1, pl.ds(size * part_at, size)]
                block = up_by(place[h], (1 - 2 * way) * (4 - step))
                mine = grads.at[w, h, block, pl.ds(size * part_at, size)]
                mine[...] = (mine[...].astype(F32) + arrived[...].astype(F32)).astype(BF16)
                rs_send(w, h, way, step + 1, part_at)

    def rs_last(w, part_at):
        size = 8 // SCATTER_PARTS[w]
        arrive(weights.at[w, :, 0, pl.ds(0, 2 * size)], rs1_r.at[w, 3, part_at])
        for h in range(2):
            mine = grads.at[w, h, place[h], pl.ds(size * part_at, size)]
            total = mine[...].astype(F32)
            for way in range(2):
                total = total + ring_in[w, h, way, 3, pl.ds(size * part_at, size)].astype(F32)
            mine[...] = total.astype(BF16)

    def rs2_send(w, part_at):
        for at in others_in(part_at, SCATTER_PARTS[w])[::-1]:
            for h in range(2):
                send(
                    grads.at[w, h, place[h], at], last_in.at[w, h, (at - 2) % 8],
                    rs2_s.at[w], rs2_r.at[5 + part_at], SUB_AXIS[h], up_by(sub_place[h], at - 1),
                )

    def rs2_ring_send(w, h, way, step):
        sign = (1 - 2 * way) * (1 - 2 * h)
        send(
            grads.at[w, h, place[h], (sign * (5 - way - step) + 1) % 8],
            last_in.at[w, h, 4 * way + step - 1],
            rs2_s.at[w], rs2_r.at[step], SUB_AXIS[h], up_by(sub_place[h], sign),
        )

    def rs2_ring_start(w):
        for h in range(2):
            for way in range(2):
                rs2_ring_send(w, h, way, 1)

    def rs2_ring_step(w, step):
        arrive(weights.at[w, 0, 0, pl.ds(0, 4)], rs2_r.at[step])
        for h in range(2):
            for way in range(2):
                if step + way < 4:
                    sign = (1 - 2 * way) * (1 - 2 * h)
                    mine = grads.at[w, h, place[h], (sign * (4 - way - step) + 1) % 8]
                    arrived = last_in[w, h, 4 * way + step - 1]
                    mine[...] = (mine[...].astype(F32) + arrived.astype(F32)).astype(BF16)
                    rs2_ring_send(w, h, way, step + 1)

    def rs_out(w, ring):
        base, out = ((down_sum, down_total_o), (up_sum, up_total_o))[w]
        if ring:
            arrive(weights.at[w, 0, 0, pl.ds(0, 2)], rs2_r.at[4])
        else:
            for part_at in range(SCATTER_PARTS[w]):
                count = len(others_in(part_at, SCATTER_PARTS[w]))
                arrive(weights.at[w, 0, pl.ds(0, 2), pl.ds(0, count)], rs2_r.at[5 + part_at])
        for h in range(2):
            total = grads[w, h, place[h], 1].astype(F32)
            for at in (3, 6) if ring else range(7):
                total = total + last_in[w, h, at].astype(F32)
            rows = pl.ds(32 * h, 32)
            out[rows, :] = base[rows, :] + total

    def block_of(h, side, j):
        return lax.rem(iz * (1 - h) + iy * h + side * (2 * j + 1) - j + 8, 8)

    def product(a, j, sides):
        w, right = ((0, cot_t), (1, late_t))[a]

        def one(h, _):
            for side in sides:
                rows = weights[w, h, block_of(h, side, j)].reshape(256, 256)
                part[a, j, pl.ds(pl.multiple_of(h * 512 + side * 256, 256), 256), :] = nn(
                    rows, right[...]
                ).astype(BF16)
            return 0

        lax.fori_loop(0, 2, one, 0)

    other = up_by(ic, 1, 2)
    my_half = pl.multiple_of(ic * 512, 512)
    other_half = pl.multiple_of(other * 512, 512)

    def s1(a, j):
        send(
            part.at[a, j, pl.ds(other_half, 512), :], pair_in.at[a, j],
            tp_s.at[a], pair_r.at[a, j], "c", other,
        )

    def s2(a, j):
        arrive(pair_in.at[a, j], pair_r.at[a, j])
        pair_sum[a, j] = (
            part[a, j, pl.ds(my_half, 512), :].astype(F32) + pair_in[a, j].astype(F32)
        ).astype(BF16)
        for step in (2, 1, 3):
            target = up_by(ix, step, 4)
            rows = pl.ds(pl.multiple_of(target * 128, 128), 128)
            send(pair_sum.at[a, j, rows, :], x_in.at[a, j, step - 1], tp_s.at[a], xr_r.at[a, j], "x", target)

    def share(a, core, x, j):
        return full.at[a, core, block_of(core, x // 2, j), pl.ds(4 * lax.rem(x, 2), 4)]

    def s3(a, j):
        total = pair_sum[a, j, pl.ds(pl.multiple_of(ix * 128, 128), 128), :].astype(F32)
        arrive(x_in.at[a, j], xr_r.at[a, j])
        for at in range(3):
            total = total + x_in[a, j, at].astype(F32)
        if a == 0:
            block = block_of(ic, ix // 2, j)
            saved = early_t[ic, block, pl.ds(4 * lax.rem(ix, 2), 4)].reshape(128, 128)
            total = total * 2.0 * jnp.maximum(saved.astype(F32), 0.0)
        ref = share(a, ic, ix, j)
        ref[...] = total.astype(BF16).reshape(4, 32, 128)
        for step in (2, 1, 3):
            send(ref, ref, tp_s.at[a], xg_r.at[a, j], "x", up_by(ix, step, 4))
        send(ref, ref, tp_s.at[a], fw_r.at[a, j], "c", other)

    def s4(a, j):
        arrive(x_in.at[a, j], xg_r.at[a, j])
        for step in (1, 2, 3):
            ref = share(a, ic, up_by(ix, step, 4), j)
            send(ref, ref, tp_s.at[a], fw_r.at[a, j], "c", other)

    def s5(a, j):
        arrive(pair_in.at[a, j], fw_r.at[a, j])

    def all_gone():
        small = weights.at[0, 0, pl.ds(0, 7), pl.ds(0, 2)]
        for w in range(2):
            gone(small, ag1_s.at[w])
            gone(small, rs2_s.at[w])
            gone(weights.at[w, :, pl.ds(0, 7)], ag2_s.at[w])
            gone(weights.at[w, :, pl.ds(0, 7)], rs1_s.at[w])
            gone(weights.at[w, :, pl.ds(0, 7)], tp_s.at[w])

    def pieces(j, fn):
        def one(at, _):
            h, side = at // 2, lax.rem(at, 2)
            fn(h, block_of(h, side, j))
            return 0

        lax.fori_loop(0, 4, one, 0)

    def up_grads(j):
        def fn(h, block):
            rows = full[0, h, block].reshape(256, 128)
            grads[1, h, block] = nn(rows, early_in[...]).astype(BF16).reshape(8, 32, 256)

        pieces(j, fn)

    def input_grads(j):
        def fn(h, block):
            acc[0] += tn(full[0, h, block].reshape(256, 128), weights[1, h, block].reshape(256, 256))

        pieces(j, fn)

    def late_outs(j):
        def fn(h, block):
            hidden = square_relu(full[1, h, block].reshape(256, 128))
            acc[1] += tn(hidden, weights[0, h, block].reshape(256, 256))

        pieces(j, fn)

    def turn_late(quarter):
        def one(at, _):
            z, y = at // 4, 2 * lax.rem(at, 4)
            rows = jnp.concatenate(
                [
                    full[1, 0, z, slot(y, 0)], full[1, 1, y, slot(z, 1)],
                    full[1, 0, z, slot(y + 1, 0)], full[1, 1, y + 1, slot(z, 1)],
                ],
                axis=0,
            )
            late_pre_o[:, pl.ds(pl.multiple_of(at * 128, 128), 128)] = rows.T
            return 0

        lax.fori_loop(8 * quarter, 8 * quarter + 8, one, 0)

    def down_grads(j):
        def fn(h, block):
            hidden = square_relu(early_t[h, block].reshape(256, 128))
            grads[0, h, block] = nn(hidden, cot[...]).astype(BF16).reshape(8, 32, 256)

        pieces(j, fn)

    def prep_late():
        late_t[...] = late_in[...].T
        acc[...] = jnp.zeros_like(acc)

    def fin_late():
        late_out_o[...] = acc[1].astype(BF16)

    def fin_input():
        input_grad_o[...] = acc[0].astype(BF16)

    own_copy(0)
    ag1_send(0)
    own_copy(1)
    prep_late()
    early(3)
    down_grads(2)
    down_grads(0)
    down_grads(3)
    rs_start(0)
    down_grads(1)
    ag1_wait(0, 0)
    ag2_start(0, 0)
    ag1_wait(0, 1)
    ag2_start(0, 1)
    ag1_ring_start(1)
    ag1_wait(0, 3)
    ag1_wait(0, 2)
    ag2_start(0, 2)
    ag2_start(0, 3)
    product(0, 0, (0,))
    ag2_part(0, 1, 0)
    ag2_part(0, 1, 1)
    ag1_ring_step(1, 1)
    ag2_start(1, 0)
    ag2_part(0, 1, 2)
    ag2_part(0, 1, 3)
    product(0, 0, (1,))
    s1(0, 0)
    product(0, 1, (0,))
    ag2_part(0, 2, 0)
    ag2_part(0, 2, 1)
    ag1_ring_step(1, 2)
    ag2_start(1, 1)
    ag2_part(0, 2, 2)
    ag2_part(0, 2, 3)
    product(0, 2, (0,))
    product(0, 1, (1,))
    s1(0, 1)
    ag2_part(1, 1, 0)
    ag2_part(0, 3, 1)
    ag1_ring_step(1, 3)
    s2(0, 1)
    s2(0, 0)
    ag2_part(1, 1, 1)
    ag2_part(0, 3, 2)
    ag2_part(0, 3, 3)
    ag2_part(0, 3, 0)
    product(0, 3, (0,))
    product(0, 2, (1,))
    s1(0, 2)
    ag2_start(1, 3)
    ag2_part(1, 2, 0)
    ag2_part(0, 4, 1)
    ag1_ring_step(1, 4)
    ag2_start(1, 2)
    product(1, 0, (0,))
    s2(0, 2)
    ag2_part(0, 4, 2)
    ag2_part(0, 4, 3)
    ag2_part(0, 4, 0)
    product(0, 3, (1,))
    s1(0, 3)
    s3(0, 0)
    ag2_part(1, 2, 1)
    rs_part(0, 1, 3)
    rs_part(0, 1, 2)
    rs_part(0, 1, 0)
    s2(0, 3)
    ag2_part(1, 1, 3)
    ag2_part(1, 1, 2)
    product(1, 0, (1,))
    product(1, 1, (0,))
    s1(1, 0)
    s3(0, 2)
    ag2_part(1, 3, 0)
    rs_part(0, 1, 1)
    rs_part(0, 2, 3)
    s4(0, 0)
    rs_part(0, 2, 0)
    rs_part(0, 2, 2)
    ag2_part(1, 2, 3)
    s3(0, 3)
    s5(0, 0)
    up_grads(0)
    ag2_part(1, 2, 2)
    product(1, 2, (0,))
    product(1, 1, (1,))
    s1(1, 1)
    s4(0, 2)
    rs_part(0, 2, 1)
    s3(0, 1)
    ag2_part(1, 4, 0)
    ag2_part(1, 3, 1)
    s2(1, 0)
    rs_part(0, 3, 3)
    s2(1, 1)
    rs_part(0, 3, 0)
    s5(0, 2)
    up_grads(2)
    rs_part(0, 3, 2)
    s4(0, 3)
    ag2_part(1, 3, 3)
    ag2_part(1, 3, 2)
    product(1, 3, (0,))
    product(1, 2, (1,))
    s5(0, 3)
    up_grads(3)
    rs_start(1)
    s1(1, 2)
    rs_part(0, 3, 1)
    s4(0, 1)
    ag2_part(1, 4, 1)
    s3(1, 0)
    rs_last(0, 3)
    rs_last(0, 0)
    s2(1, 2)
    s5(0, 1)
    up_grads(1)
    rs_last(0, 2)
    ag2_part(1, 4, 3)
    ag2_part(1, 4, 2)
    input_grads(1)
    rs_part(1, 1, 2)
    s3(1, 1)
    rs_part(1, 1, 1)
    input_grads(3)
    rs_part(1, 1, 3)
    product(1, 3, (1,))
    s1(1, 3)
    rs_part(1, 1, 0)
    input_grads(2)
    s4(1, 0)
    input_grads(0)
    s2(1, 3)
    s3(1, 2)
    rs_last(0, 1)
    rs2_ring_start(0)
    fin_input()
    rs_part(1, 2, 2)
    s5(1, 0)
    late_outs(0)
    rs_part(1, 2, 3)
    s4(1, 1)
    rs_part(1, 2, 0)
    rs_part(1, 2, 1)
    s5(1, 1)
    late_outs(1)
    rs2_ring_step(0, 1)
    rs_part(1, 3, 2)
    s3(1, 3)
    rs_part(1, 3, 3)
    rs_part(1, 3, 0)
    s4(1, 2)
    rs_part(1, 3, 1)
    rs2_ring_step(0, 2)
    s5(1, 2)
    late_outs(2)
    rs_last(1, 2)
    rs2_send(1, 2)
    rs_last(1, 3)
    rs2_send(1, 3)
    s4(1, 3)
    rs_last(1, 0)
    rs2_send(1, 0)
    rs_last(1, 1)
    rs2_send(1, 1)
    s5(1, 3)
    turn_late(2)
    rs2_ring_step(0, 3)
    turn_late(0)
    late_outs(3)
    fin_late()
    turn_late(1)
    turn_late(3)
    rs_out(1, False)
    rs_out(0, True)
    all_gone()


def deliver(*refs):
    sources, targets, sems = refs[:5], refs[5:10], refs[10]
    copies = [pltpu.make_async_copy(a, b, sems.at[at]) for at, (a, b) in enumerate(zip(sources, targets))]
    for copy in copies:
        copy.start()
    for copy in copies:
        copy.wait()


def body(late_input, up_weight, down_weight, early_input, early_pre, cotangent, up_sum, down_sum):
    vmem = pl.BlockSpec(memory_space=pltpu.VMEM)
    anywhere = pl.BlockSpec(memory_space=pl.ANY)
    dma = pltpu.SemaphoreType.DMA
    results = (((128, 4096), BF16), ((128, 256), BF16), ((128, 256), BF16), ((64, 256), F32), ((64, 256), F32))
    held = pl.pallas_call(
        kernel,
        out_shape=tuple(pltpu.VMEM(shape, dtype) for shape, dtype in results),
        in_specs=[anywhere] * 8,
        out_specs=(vmem,) * 5,
        scratch_shapes=[
            pltpu.VMEM((128, 256), BF16),
            pltpu.VMEM((64, 256), BF16),
            pltpu.VMEM((64, 256), BF16),
            pltpu.VMEM((128, 256), BF16),
            pltpu.VMEM((128, 4096), BF16),
            pltpu.VMEM((128, 256), BF16),
            pltpu.VMEM((64, 256), F32),
            pltpu.VMEM((64, 256), F32),
            pltpu.VMEM((2, 2, 8, 8, 32, 256), BF16),
            pltpu.VMEM((2, 2, 8, 8, 32, 256), BF16),
            pltpu.VMEM((2, 2, 2, 4, 8, 32, 256), BF16),
            pltpu.VMEM((2, 2, 7, 32, 256), BF16),
            pltpu.VMEM((2, 8, 8, 32, 128), BF16),
            pltpu.VMEM((256, 128), BF16),
            pltpu.VMEM((256, 128), BF16),
            pltpu.VMEM((2, 4, 1024, 128), BF16),
            pltpu.VMEM((2, 4, 512, 128), BF16),
            pltpu.VMEM((2, 4, 512, 128), BF16),
            pltpu.VMEM((2, 4, 3, 128, 128), BF16),
            pltpu.VMEM((2, 2, 8, 8, 32, 128), BF16),
            pltpu.VMEM((2, 128, 256), F32),
            dma((4,)), dma((2,)),
            dma((2,)), dma((9,)),
            dma((2,)), dma((2, 4, 4)),
            dma((2,)), dma((2, 4, 4)),
            dma((2,)), dma((9,)),
            dma((2,)), dma((2, 4)), dma((2, 4)), dma((2, 4)), dma((2, 4)),
        ],
        compiler_params=pltpu.CompilerParams(
            collective_id=0, has_side_effects=True, vmem_limit_bytes=36 * 1024 * 1024
        ),
        cost_estimate=pl.CostEstimate(flops=1_700_000_000, bytes_accessed=8_000_000, transcendentals=0),
    )(*(
        pltpu.with_memory_space_constraint(value, pltpu.MemorySpace.HBM)
        for value in (
            late_input, up_weight.T, down_weight, early_input, early_pre, cotangent, up_sum.T, down_sum
        )
    ))
    outs = pl.pallas_call(
        deliver,
        out_shape=tuple(jax.ShapeDtypeStruct(shape, dtype) for shape, dtype in results),
        in_specs=[vmem] * 5,
        out_specs=(anywhere,) * 5,
        scratch_shapes=[dma((5,))],
        compiler_params=pltpu.CompilerParams(vmem_limit_bytes=8 * 1024 * 1024),
    )(*held)
    late_pre, late_out, input_grad, up_total, down_total = outs
    return late_pre, late_out, input_grad, up_total.T, down_total


def solution(mesh):
    split = Mesh(mesh.devices.reshape(8, 8, 4, 2), FS + TP)
    placed = (
        P(FS, TP), P(TP, FS), P(FS, TP), P(FS, TP), P(FS, None), P(FS, TP), P(TP, FS), P(FS, TP),
    )
    return jax.shard_map(
        body,
        mesh=split,
        in_specs=placed,
        out_specs=(P(FS, None), P(FS, TP), P(FS, TP), P(TP, FS), P(FS, TP)),
        check_vma=False,
    )
```

```python
import jax
import jax.numpy as jnp
from jax import lax
from jax.experimental import pallas as pl
from jax.experimental.pallas import tpu as pltpu
from jax.sharding import Mesh
from jax.sharding import PartitionSpec as P

FS = ("z", "y")
TP = ("x", "c")
MESH = pl.DeviceIdType.MESH
F32 = jnp.float32
BF16 = jnp.bfloat16
BLOCK_AXIS = ("z", "y")
SUB_AXIS = ("y", "z")
GATHER_PARTS = (4, 4)
SCATTER_PARTS = (4, 4)


def nn(left, right):
    return lax.dot_general(left, right, (((1,), (0,)), ((), ())), preferred_element_type=F32)


def tn(left, right):
    return lax.dot_general(left, right, (((0,), (0,)), ((), ())), preferred_element_type=F32)


def square_relu(value):
    return jnp.square(jnp.maximum(value.astype(F32), 0.0)).astype(BF16)


def kernel(
    late_in_h, up_t_h, down_h, early_in_h, early_pre_h, cot_h, up_sum_h, down_sum_h,
    late_pre_o, late_out_o, input_grad_o, up_total_o, down_total_o,
    late_in, up_t, down, early_in, early_pre, cot, up_sum, down_sum,
    weights, grads, ring_in, last_in, early_t, cot_t, late_t, part, pair_in, pair_sum, x_in, full, acc,
    in_sem, own_sem, ag1_s, ag1_r, ag2_s, ag2_r, rs1_s, rs1_r, rs2_s, rs2_r,
    tp_s, pair_r, xr_r, xg_r, fw_r,
):
    iz, iy, ix, ic = (lax.axis_index(name) for name in ("z", "y", "x", "c"))
    place = (iz, iy)
    sub_place = (iy, iz)
    shards = (down, up_t)

    def up_by(value, step, size=8):
        return lax.rem(value + (step % size), size)

    def send(src, dst, send_sem, recv_sem, axis, index):
        pltpu.make_async_remote_copy(
            src_ref=src, dst_ref=dst, send_sem=send_sem, recv_sem=recv_sem,
            device_id={axis: index}, device_id_type=MESH,
        ).start()

    def arrive(ref, recv_sem):
        pltpu.make_async_remote_copy(
            src_ref=ref, dst_ref=ref, send_sem=recv_sem, recv_sem=recv_sem,
            device_id={"c": up_by(ic, 1, 2)}, device_id_type=MESH,
        ).wait_recv()

    def gone(ref, send_sem):
        pltpu.make_async_remote_copy(
            src_ref=ref, dst_ref=ref, send_sem=send_sem, recv_sem=send_sem,
            device_id={"c": up_by(ic, 1, 2)}, device_id_type=MESH,
        ).wait_send()

    barrier = pltpu.get_barrier_semaphore()
    steps = [(step, axis, me, 8) for step in (4, 5, 3, 6, 2, 7, 1) for axis, me in (("z", iz), ("y", iy))]
    steps += [(step, "x", ix, 4) for step in (2, 1, 3)] + [(1, "c", ic, 2)]
    for step, axis, me, size in steps:
        pl.semaphore_signal(
            barrier, inc=1, device_id={axis: up_by(me, step, size)}, device_id_type=MESH
        )
    loads = []
    for at, source, target in (
        (0, down_h, down), (1, cot_h, cot), (2, early_pre_h, early_pre), (3, up_t_h, up_t), (3, late_in_h, late_in),
        (3, early_in_h, early_in), (3, down_sum_h, down_sum), (3, up_sum_h, up_sum),
    ):
        copy = pltpu.make_async_copy(source, target, in_sem.at[at])
        copy.start()
        loads.append(copy)
    def slot(sub, h):
        return lax.rem(sub - sub_place[h] + 9, 8)

    def early(quarter):
        def one(at, _):
            z, y = at // 4, 2 * lax.rem(at, 4)
            turned = early_pre[:, pl.ds(pl.multiple_of(at * 128, 128), 128)].T
            early_t[0, z, slot(y, 0)] = turned[0:32]
            early_t[1, y, slot(z, 1)] = turned[32:64]
            early_t[0, z, slot(y + 1, 0)] = turned[64:96]
            early_t[1, y + 1, slot(z, 1)] = turned[96:128]
            return 0

        lax.fori_loop(8 * quarter, 8 * quarter + 8, one, 0)

    loads[1].wait()
    cot_t[...] = cot[...].T
    loads[2].wait()
    early(0)
    early(1)
    early(2)
    loads[0].wait()
    pl.semaphore_wait(barrier, 18)

    def own_copy(w):
        if w == 1:
            rest = weights.at[:, 1, pl.ds(0, 3), pl.ds(0, 3)]
            pltpu.make_async_copy(rest, rest, in_sem.at[3]).wait()
        for h in range(2):
            rows = shards[w].at[pl.ds(32 * h, 32), :]
            pltpu.make_async_copy(rows, weights.at[w, h, place[h], 1], own_sem.at[w]).start()

    def own_wait(w):
        both = weights.at[w, :, 0, 0]
        pltpu.make_async_copy(both, both, own_sem.at[w]).wait()

    def others_in(part_at, parts):
        slots = range(part_at * 8 // parts, (part_at + 1) * 8 // parts)
        return [at for at in slots if at != 1]

    def ag1_send(w):
        for part_at in range(GATHER_PARTS[w]):
            for at in others_in(part_at, GATHER_PARTS[w])[::-1]:
                for h in range(2):
                    send(
                        shards[w].at[pl.ds(32 * h, 32), :], weights.at[w, h, place[h], at],
                        ag1_s.at[w], ag1_r.at[5 + part_at], SUB_AXIS[h], up_by(sub_place[h], 1 - at),
                    )

    def ag1_wait(w, part_at):
        if part_at == 0:
            own_wait(w)
        count = len(others_in(part_at, GATHER_PARTS[w]))
        arrive(weights.at[w, 0, pl.ds(0, 2), pl.ds(0, count)], ag1_r.at[5 + part_at])

    def ring_send(w, h, way, step):
        sign = (1 - 2 * way) * (1 - 2 * h)
        ref = weights.at[w, h, place[h], (9 - sign * (step - 1)) % 8]
        target = weights.at[w, h, place[h], (9 - sign * step) % 8]
        send(ref, target, ag1_s.at[w], ag1_r.at[step], SUB_AXIS[h], up_by(sub_place[h], sign))

    def ag1_ring_start(w):
        own_wait(w)
        for h in range(2):
            for way in range(2):
                ring_send(w, h, way, 1)

    def ag1_ring_step(w, step):
        arrive(weights.at[w, 0, 0, pl.ds(0, 4 if step < 4 else 2)], ag1_r.at[step])
        for h in range(2):
            for way in range(2):
                if step + way < 4:
                    ring_send(w, h, way, step + 1)

    def ag2_send(w, h, way, step, part_at):
        sign = 1 - 2 * way
        size = 8 // GATHER_PARTS[w]
        ref = weights.at[w, h, up_by(place[h], -sign * (step - 1)), pl.ds(size * part_at, size)]
        send(ref, ref, ag2_s.at[w], ag2_r.at[w, step - 1, part_at], BLOCK_AXIS[h], up_by(place[h], sign))

    def ag2_start(w, part_at):
        for h in range(2):
            for way in range(2):
                ag2_send(w, h, way, 1, part_at)

    def ag2_part(w, step, part_at):
        parts = GATHER_PARTS[w]
        size = (16 if step < 4 else 8) // parts
        arrive(weights.at[w, :, 0, pl.ds(0, size)], ag2_r.at[w, step - 1, part_at])
        for h in range(2):
            for way in range(2):
                if step < 3 or (step == 3 and 2 * part_at // parts == way):
                    ag2_send(w, h, way, step + 1, part_at)

    def rs_send(w, h, way, step, part_at):
        sign = 1 - 2 * way
        size = 8 // SCATTER_PARTS[w]
        send(
            grads.at[w, h, up_by(place[h], sign * (5 - step)), pl.ds(size * part_at, size)],
            ring_in.at[w, h, way, step - 1, pl.ds(size * part_at, size)],
            rs1_s.at[w], rs1_r.at[w, step - 1, part_at], BLOCK_AXIS[h], up_by(place[h], sign),
        )

    def rs_start(w):
        parts = SCATTER_PARTS[w]
        for step in (1, 2):
            for part_at in ((1, 0), (2, 3, 1, 0))[parts // 4]:
                way = (2 * part_at // parts + step - 1) % 2
                for h in range(2):
                    rs_send(w, h, way, step, part_at)

    def rs_part(w, step, part_at):
        parts = SCATTER_PARTS[w]
        size = 8 // parts
        arrive(weights.at[w, :, 0, pl.ds(0, 2 * size if step > 1 else size)], rs1_r.at[w, step - 1, part_at])
        for h in range(2):
            for way in range(2):
                if step == 1 and 2 * part_at // parts != way:
                    continue
                arrived = ring_in.at[w, h, way, step - 1, pl.ds(size * part_at, size)]
                block = up_by(place[h], (1 - 2 * way) * (4 - step))
                mine = grads.at[w, h, block, pl.ds(size * part_at, size)]
                mine[...] = (mine[...].astype(F32) + arrived[...].astype(F32)).astype(BF16)
                rs_send(w, h, way, step + 1, part_at)

    def rs_last(w, part_at):
        size = 8 // SCATTER_PARTS[w]
        arrive(weights.at[w, :, 0, pl.ds(0, 2 * size)], rs1_r.at[w, 3, part_at])
        for h in range(2):
            mine = grads.at[w, h, place[h], pl.ds(size * part_at, size)]
            total = mine[...].astype(F32)
            for way in range(2):
                total = total + ring_in[w, h, way, 3, pl.ds(size * part_at, size)].astype(F32)
            mine[...] = total.astype(BF16)

    def rs2_send(w, part_at):
        for at in others_in(part_at, SCATTER_PARTS[w])[::-1]:
            for h in range(2):
                send(
                    grads.at[w, h, place[h], at], last_in.at[w, h, (at - 2) % 8],
                    rs2_s.at[w], rs2_r.at[5 + part_at], SUB_AXIS[h], up_by(sub_place[h], at - 1),
                )

    def rs2_ring_send(w, h, way, step):
        sign = (1 - 2 * way) * (1 - 2 * h)
        send(
            grads.at[w, h, place[h], (sign * (5 - way - step) + 1) % 8],
            last_in.at[w, h, 4 * way + step - 1],
            rs2_s.at[w], rs2_r.at[step], SUB_AXIS[h], up_by(sub_place[h], sign),
        )

    def rs2_ring_start(w):
        for h in range(2):
            for way in range(2):
                rs2_ring_send(w, h, way, 1)

    def rs2_ring_step(w, step):
        arrive(weights.at[w, 0, 0, pl.ds(0, 4)], rs2_r.at[step])
        for h in range(2):
            for way in range(2):
                if step + way < 4:
                    sign = (1 - 2 * way) * (1 - 2 * h)
                    mine = grads.at[w, h, place[h], (sign * (4 - way - step) + 1) % 8]
                    arrived = last_in[w, h, 4 * way + step - 1]
                    mine[...] = (mine[...].astype(F32) + arrived.astype(F32)).astype(BF16)
                    rs2_ring_send(w, h, way, step + 1)

    def rs_out(w, ring):
        base, out = ((down_sum, down_total_o), (up_sum, up_total_o))[w]
        if ring:
            arrive(weights.at[w, 0, 0, pl.ds(0, 2)], rs2_r.at[4])
        else:
            for part_at in range(SCATTER_PARTS[w]):
                count = len(others_in(part_at, SCATTER_PARTS[w]))
                arrive(weights.at[w, 0, pl.ds(0, 2), pl.ds(0, count)], rs2_r.at[5 + part_at])
        for h in range(2):
            total = grads[w, h, place[h], 1].astype(F32)
            for at in (3, 6) if ring else range(7):
                total = total + last_in[w, h, at].astype(F32)
            rows = pl.ds(32 * h, 32)
            out[rows, :] = base[rows, :] + total

    def block_of(h, side, j):
        return lax.rem(iz * (1 - h) + iy * h + side * (2 * j + 1) - j + 8, 8)

    def product(a, j, sides):
        w, right = ((0, cot_t), (1, late_t))[a]

        def one(h, _):
            for side in sides:
                rows = weights[w, h, block_of(h, side, j)].reshape(256, 256)
                part[a, j, pl.ds(pl.multiple_of(h * 512 + side * 256, 256), 256), :] = nn(
                    rows, right[...]
                ).astype(BF16)
            return 0

        lax.fori_loop(0, 2, one, 0)

    other = up_by(ic, 1, 2)
    my_half = pl.multiple_of(ic * 512, 512)
    other_half = pl.multiple_of(other * 512, 512)

    def s1(a, j):
        send(
            part.at[a, j, pl.ds(other_half, 512), :], pair_in.at[a, j],
            tp_s.at[a], pair_r.at[a, j], "c", other,
        )

    def s2(a, j):
        arrive(pair_in.at[a, j], pair_r.at[a, j])
        pair_sum[a, j] = (
            part[a, j, pl.ds(my_half, 512), :].astype(F32) + pair_in[a, j].astype(F32)
        ).astype(BF16)
        for step in (2, 1, 3):
            target = up_by(ix, step, 4)
            rows = pl.ds(pl.multiple_of(target * 128, 128), 128)
            send(pair_sum.at[a, j, rows, :], x_in.at[a, j, step - 1], tp_s.at[a], xr_r.at[a, j], "x", target)

    def share(a, core, x, j):
        return full.at[a, core, block_of(core, x // 2, j), pl.ds(4 * lax.rem(x, 2), 4)]

    def s3(a, j):
        total = pair_sum[a, j, pl.ds(pl.multiple_of(ix * 128, 128), 128), :].astype(F32)
        arrive(x_in.at[a, j], xr_r.at[a, j])
        for at in range(3):
            total = total + x_in[a, j, at].astype(F32)
        if a == 0:
            block = block_of(ic, ix // 2, j)
            saved = early_t[ic, block, pl.ds(4 * lax.rem(ix, 2), 4)].reshape(128, 128)
            total = total * 2.0 * jnp.maximum(saved.astype(F32), 0.0)
        ref = share(a, ic, ix, j)
        ref[...] = total.astype(BF16).reshape(4, 32, 128)
        for step in (2, 1, 3):
            send(ref, ref, tp_s.at[a], xg_r.at[a, j], "x", up_by(ix, step, 4))
        send(ref, ref, tp_s.at[a], fw_r.at[a, j], "c", other)

    def s4(a, j):
        arrive(x_in.at[a, j], xg_r.at[a, j])
        for step in (1, 2, 3):
            ref = share(a, ic, up_by(ix, step, 4), j)
            send(ref, ref, tp_s.at[a], fw_r.at[a, j], "c", other)

    def s5(a, j):
        arrive(pair_in.at[a, j], fw_r.at[a, j])

    def all_gone():
        small = weights.at[0, 0, pl.ds(0, 7), pl.ds(0, 2)]
        for w in range(2):
            gone(small, ag1_s.at[w])
            gone(small, rs2_s.at[w])
            gone(weights.at[w, :, pl.ds(0, 7)], ag2_s.at[w])
            gone(weights.at[w, :, pl.ds(0, 7)], rs1_s.at[w])
            gone(weights.at[w, :, pl.ds(0, 7)], tp_s.at[w])

    def pieces(j, fn):
        def one(at, _):
            h, side = at // 2, lax.rem(at, 2)
            fn(h, block_of(h, side, j))
            return 0

        lax.fori_loop(0, 4, one, 0)

    def up_grads(j):
        def fn(h, block):
            rows = full[0, h, block].reshape(256, 128)
            grads[1, h, block] = nn(rows, early_in[...]).astype(BF16).reshape(8, 32, 256)

        pieces(j, fn)

    def input_grads(j):
        def fn(h, block):
            acc[0] += tn(full[0, h, block].reshape(256, 128), weights[1, h, block].reshape(256, 256))

        pieces(j, fn)

    def late_outs(j):
        def fn(h, block):
            hidden = square_relu(full[1, h, block].reshape(256, 128))
            acc[1] += tn(hidden, weights[0, h, block].reshape(256, 256))

        pieces(j, fn)

    def turn_late(quarter):
        def one(at, _):
            z, y = at // 4, 2 * lax.rem(at, 4)
            rows = jnp.concatenate(
                [
                    full[1, 0, z, slot(y, 0)], full[1, 1, y, slot(z, 1)],
                    full[1, 0, z, slot(y + 1, 0)], full[1, 1, y + 1, slot(z, 1)],
                ],
                axis=0,
            )
            late_pre_o[:, pl.ds(pl.multiple_of(at * 128, 128), 128)] = rows.T
            return 0

        lax.fori_loop(8 * quarter, 8 * quarter + 8, one, 0)

    def down_grads(j):
        def fn(h, block):
            hidden = square_relu(early_t[h, block].reshape(256, 128))
            grads[0, h, block] = nn(hidden, cot[...]).astype(BF16).reshape(8, 32, 256)

        pieces(j, fn)

    def prep_late():
        late_t[...] = late_in[...].T
        acc[...] = jnp.zeros_like(acc)

    def fin_late():
        late_out_o[...] = acc[1].astype(BF16)

    def fin_input():
        input_grad_o[...] = acc[0].astype(BF16)

    own_copy(0)
    ag1_send(0)
    early(3)
    down_grads(3)
    down_grads(2)
    own_copy(1)
    rs_start(0)
    down_grads(0)
    prep_late()
    down_grads(1)
    ag1_wait(0, 0)
    ag2_start(0, 0)
    ag1_wait(0, 1)
    ag2_start(0, 1)
    ag1_ring_start(1)
    ag1_wait(0, 3)
    ag1_wait(0, 2)
    ag2_start(0, 2)
    ag2_start(0, 3)
    product(0, 0, (0,))
    ag2_part(0, 1, 0)
    ag2_part(0, 1, 1)
    ag1_ring_step(1, 1)
    ag2_start(1, 0)
    ag2_part(0, 1, 2)
    ag2_part(0, 1, 3)
    product(0, 1, (0,))
    product(0, 0, (1,))
    s1(0, 0)
    ag2_part(0, 2, 0)
    ag2_part(0, 2, 1)
    ag1_ring_step(1, 2)
    ag2_start(1, 1)
    s2(0, 0)
    ag2_part(0, 2, 2)
    ag2_part(0, 2, 3)
    product(0, 1, (1,))
    product(0, 2, (0,))
    s1(0, 1)
    ag2_part(1, 1, 0)
    ag2_part(0, 3, 1)
    s2(0, 1)
    ag1_ring_step(1, 3)
    ag2_part(1, 1, 1)
    ag2_part(0, 3, 2)
    s3(0, 0)
    ag2_part(0, 3, 0)
    ag2_part(0, 3, 3)
    product(0, 2, (1,))
    product(0, 3, (0,))
    ag2_part(1, 2, 0)
    s1(0, 2)
    ag2_part(0, 4, 1)
    ag1_ring_step(1, 4)
    ag2_start(1, 2)
    ag2_start(1, 3)
    product(1, 0, (0,))
    s2(0, 2)
    s3(0, 1)
    ag2_part(1, 2, 1)
    ag2_part(0, 4, 2)
    ag2_part(0, 4, 0)
    ag2_part(0, 4, 3)
    rs_part(0, 1, 1)
    rs_part(0, 1, 2)
    product(0, 3, (1,))
    s1(0, 3)
    rs_part(0, 1, 3)
    s4(0, 0)
    ag2_part(1, 3, 0)
    rs_part(0, 1, 0)
    s2(0, 3)
    ag2_part(1, 1, 2)
    s5(0, 0)
    up_grads(0)
    ag2_part(1, 1, 3)
    product(1, 0, (1,))
    s1(1, 0)
    product(1, 1, (0,))
    s3(0, 2)
    rs_part(0, 2, 1)
    rs_part(0, 2, 2)
    s4(0, 1)
    s2(1, 0)
    ag2_part(1, 4, 0)
    rs_part(0, 2, 3)
    rs_part(0, 2, 0)
    s5(0, 1)
    up_grads(1)
    s3(0, 3)
    ag2_part(1, 2, 2)
    ag2_part(1, 2, 3)
    product(1, 2, (0,))
    product(1, 1, (1,))
    rs_part(0, 3, 1)
    s1(1, 1)
    s4(0, 2)
    ag2_part(1, 3, 1)
    rs_part(0, 3, 2)
    s2(1, 1)
    rs_part(0, 3, 3)
    s5(0, 2)
    up_grads(2)
    s3(1, 0)
    rs_part(0, 3, 0)
    ag2_part(1, 3, 2)
    s4(0, 3)
    ag2_part(1, 3, 3)
    product(1, 3, (0,))
    product(1, 2, (1,))
    s1(1, 2)
    rs_last(0, 1)
    s5(0, 3)
    up_grads(3)
    ag2_part(1, 4, 1)
    rs_start(1)
    s3(1, 1)
    rs_last(0, 2)
    s2(1, 2)
    rs_last(0, 3)
    s4(1, 0)
    ag2_part(1, 4, 2)
    rs_last(0, 0)
    rs2_ring_start(0)
    ag2_part(1, 4, 3)
    product(1, 3, (1,))
    s1(1, 3)
    input_grads(1)
    s5(1, 0)
    rs_part(1, 1, 2)
    late_outs(0)
    rs_part(1, 1, 3)
    rs_part(1, 1, 0)
    rs_part(1, 1, 1)
    input_grads(0)
    s4(1, 1)
    input_grads(3)
    rs2_ring_step(0, 1)
    s2(1, 3)
    s3(1, 2)
    input_grads(2)
    rs_part(1, 2, 2)
    s5(1, 1)
    late_outs(1)
    rs_part(1, 2, 3)
    fin_input()
    rs_part(1, 2, 1)
    rs2_ring_step(0, 2)
    rs_part(1, 2, 0)
    rs_part(1, 3, 2)
    s3(1, 3)
    rs_part(1, 3, 3)
    s4(1, 2)
    rs_part(1, 3, 1)
    rs2_ring_step(0, 3)
    rs_part(1, 3, 0)
    s5(1, 2)
    late_outs(2)
    rs_last(1, 2)
    rs2_send(1, 2)
    rs_last(1, 3)
    rs2_send(1, 3)
    s4(1, 3)
    rs_last(1, 1)
    rs2_send(1, 1)
    rs_out(0, True)
    s5(1, 3)
    turn_late(1)
    rs_last(1, 0)
    rs2_send(1, 0)
    turn_late(3)
    turn_late(2)
    late_outs(3)
    fin_late()
    turn_late(0)
    rs_out(1, False)
    all_gone()


def deliver(*refs):
    sources, targets, sems = refs[:5], refs[5:10], refs[10]
    copies = [pltpu.make_async_copy(a, b, sems.at[at]) for at, (a, b) in enumerate(zip(sources, targets))]
    for copy in copies:
        copy.start()
    for copy in copies:
        copy.wait()


def body(late_input, up_weight, down_weight, early_input, early_pre, cotangent, up_sum, down_sum):
    vmem = pl.BlockSpec(memory_space=pltpu.VMEM)
    anywhere = pl.BlockSpec(memory_space=pl.ANY)
    dma = pltpu.SemaphoreType.DMA
    results = (((128, 4096), BF16), ((128, 256), BF16), ((128, 256), BF16), ((64, 256), F32), ((64, 256), F32))
    held = pl.pallas_call(
        kernel,
        out_shape=tuple(pltpu.VMEM(shape, dtype) for shape, dtype in results),
        in_specs=[anywhere] * 8,
        out_specs=(vmem,) * 5,
        scratch_shapes=[
            pltpu.VMEM((128, 256), BF16),
            pltpu.VMEM((64, 256), BF16),
            pltpu.VMEM((64, 256), BF16),
            pltpu.VMEM((128, 256), BF16),
            pltpu.VMEM((128, 4096), BF16),
            pltpu.VMEM((128, 256), BF16),
            pltpu.VMEM((64, 256), F32),
            pltpu.VMEM((64, 256), F32),
            pltpu.VMEM((2, 2, 8, 8, 32, 256), BF16),
            pltpu.VMEM((2, 2, 8, 8, 32, 256), BF16),
            pltpu.VMEM((2, 2, 2, 4, 8, 32, 256), BF16),
            pltpu.VMEM((2, 2, 7, 32, 256), BF16),
            pltpu.VMEM((2, 8, 8, 32, 128), BF16),
            pltpu.VMEM((256, 128), BF16),
            pltpu.VMEM((256, 128), BF16),
            pltpu.VMEM((2, 4, 1024, 128), BF16),
            pltpu.VMEM((2, 4, 512, 128), BF16),
            pltpu.VMEM((2, 4, 512, 128), BF16),
            pltpu.VMEM((2, 4, 3, 128, 128), BF16),
            pltpu.VMEM((2, 2, 8, 8, 32, 128), BF16),
            pltpu.VMEM((2, 128, 256), F32),
            dma((4,)), dma((2,)),
            dma((2,)), dma((9,)),
            dma((2,)), dma((2, 4, 4)),
            dma((2,)), dma((2, 4, 4)),
            dma((2,)), dma((9,)),
            dma((2,)), dma((2, 4)), dma((2, 4)), dma((2, 4)), dma((2, 4)),
        ],
        compiler_params=pltpu.CompilerParams(
            collective_id=0, has_side_effects=True, vmem_limit_bytes=36 * 1024 * 1024
        ),
        cost_estimate=pl.CostEstimate(flops=1_700_000_000, bytes_accessed=8_000_000, transcendentals=0),
    )(*(
        pltpu.with_memory_space_constraint(value, pltpu.MemorySpace.HBM)
        for value in (
            late_input, up_weight.T, down_weight, early_input, early_pre, cotangent, up_sum.T, down_sum
        )
    ))
    outs = pl.pallas_call(
        deliver,
        out_shape=tuple(jax.ShapeDtypeStruct(shape, dtype) for shape, dtype in results),
        in_specs=[vmem] * 5,
        out_specs=(anywhere,) * 5,
        scratch_shapes=[dma((5,))],
        compiler_params=pltpu.CompilerParams(vmem_limit_bytes=8 * 1024 * 1024),
    )(*held)
    late_pre, late_out, input_grad, up_total, down_total = outs
    return late_pre, late_out, input_grad, up_total.T, down_total


def solution(mesh):
    split = Mesh(mesh.devices.reshape(8, 8, 4, 2), FS + TP)
    placed = (
        P(FS, TP), P(TP, FS), P(FS, TP), P(FS, TP), P(FS, None), P(FS, TP), P(TP, FS), P(FS, TP),
    )
    return jax.shard_map(
        body,
        mesh=split,
        in_specs=placed,
        out_specs=(P(FS, None), P(FS, TP), P(FS, TP), P(TP, FS), P(FS, TP)),
        check_vma=False,
    )
```
